32 devices in a mesh: kv: 8 (over z, y), tp: 4 (over x, core).
Axes of the slice: x: 2, y: 2, z: 4, core: 2. Of those that a mesh axis runs over, the one named last changes fastest.
Arguments:
- tokens: bfloat16 [5120, 4096], P('kv'), may hold values from -48 to 48
- query_weight: bfloat16 [4096, 2048], P(None, 'tp'), may hold values from -0.09375 to 0.09375
- key_weight: bfloat16 [4096, 512], P(None, 'tp'), may hold values from -0.09375 to 0.09375
- value_weight: bfloat16 [4096, 512], P(None, 'tp'), may hold values from -0.09375 to 0.09375
- gate_weight: bfloat16 [4096, 64], replicated, may hold values from -0.09375 to 0.09375
- summary_pos: bfloat16 [32, 64], replicated, may hold values from -6 to 6
- key_mixing: bfloat16 [32, 8], replicated, may hold values from -1 to 1
- value_mixing: bfloat16 [32, 8], replicated, may hold values from -1 to 1
- out_weight: bfloat16 [2048, 4096], P('tp'), may hold values from -0.125 to 0.125
- chosen: int32 [80, 8, 16], P('kv', 'tp'), may hold values from 0 to 79, as said below
Outputs:
- mixed: bfloat16 [5120, 4096], P(('kv', 'tp'))
The draws below stay inside these ranges and needn't reach their ends.
Inputs may be any that keep to these rules, and one draw needn't show every extreme that they name: `chosen`: entry [b, g, 0] is b itself; every entry is at most b. For the query blocks of one index of kv, one key head and any OTHER index of kv, at most 2 distinct blocks of that index's 64-position blocks are named, and exactly 2 of the index just before. Entries may repeat.
All inputs are finite; a program needn't handle non-finite values.
Results may differ from the reference program's by a relative error of at most 0.013.
The reference program's roundings to bfloat16 on the way count: a program that leaves them out, or rounds other values in their place, can miss the bound.
Values may be sent and summed in bfloat16 or wider, within the bound.
No kernel may reach another device: no remote copies, remote signals or barrier semaphores. Data moves between devices by JAX's collectives and lax.ppermute only.
A program may use at most 192 MiB of HBM per device.

```python
import jax
import jax.numpy as jnp
from jax import lax

D = 4096
HEADS = 32
KV_HEADS = 8
HD = 64
CMP = 32
SB = 64
N_SEL = 16
CAP = 2
TOK_DEV = 640
TOKENS = 5120
N_TP = 4


def draw_tokens(key, part):
    base = jax.random.normal(key, (TOKENS, D), jnp.float32)
    return jnp.clip(base, -6.0, 6.0).astype(jnp.bfloat16)


def draw_chosen(key, part):
    per_device = TOK_DEV // SB
    block_total = TOKENS // SB
    device_total = block_total // per_device
    grid_shape = (block_total, KV_HEADS, N_SEL)
    column_shape = (block_total, KV_HEADS, 1)
    streams = jax.random.split(key, 8)
    query_block = jnp.arange(block_total, dtype=jnp.int32)[:, None, None]
    device_of = query_block // per_device
    head_ids = jnp.arange(KV_HEADS, dtype=jnp.int32)[None, :, None]
    first_pick = jax.random.randint(streams[0], (device_total, KV_HEADS, device_total), 0, per_device)
    pick_step = jax.random.randint(streams[1], (device_total, KV_HEADS, device_total), 1, per_device)
    popular = jax.random.randint(streams[2], (4,), 0, device_total)
    use_popular = jax.random.randint(streams[3], grid_shape, 0, 2)
    popular_pick = popular[jax.random.randint(streams[4], grid_shape, 0, 4)]
    drawn_pick = jax.random.randint(streams[5], grid_shape, 0, device_of + 1)
    source = jnp.where((use_popular == 1) & (popular_pick <= device_of), popular_pick, drawn_pick)
    which = jax.random.randint(streams[6], grid_shape, 0, CAP)
    candidate = (first_pick[device_of, head_ids, source] + which * pick_step[device_of, head_ids, source]) % per_device
    at_home = jax.random.randint(streams[7], grid_shape, device_of * per_device, query_block + 1)
    picks = jnp.where(source == device_of, at_home, source * per_device + candidate)
    before = jnp.maximum(device_of - 1, 0)
    half_away = jnp.maximum(device_of - device_total // 2, 0)
    first_before = first_pick[device_of, head_ids, before]
    own_block = jnp.broadcast_to(query_block, column_shape)
    slot_one = jnp.where(device_of >= 1, before * per_device + first_before, own_block)
    slot_two = jnp.where(device_of >= device_total // 2, half_away * per_device + first_pick[device_of, head_ids, half_away], own_block)
    slot_three = jnp.where(device_of >= 1, before * per_device + (first_before + pick_step[device_of, head_ids, before]) % per_device, own_block)
    return jnp.concatenate([own_block, jnp.broadcast_to(slot_one, column_shape), jnp.broadcast_to(slot_two, column_shape), jnp.broadcast_to(slot_three, column_shape), picks[:, :, 4:]], axis=2).astype(jnp.int32)


def shard_levels(stream_key, shape, pieces, smallest, high):
    def one(position, shards_of):
        draws = jax.random.uniform(jax.random.fold_in(jax.random.fold_in(stream_key, 6), position), (shards_of,), jnp.float32, smallest / len(pieces), high / len(pieces))
        return jnp.repeat(jnp.exp(draws), shape[position] // shards_of).reshape((-1,) + (1,) * (len(shape) - position - 1))

    gain = one(*pieces[0])
    for cut in pieces[1:]:
        gain = gain * one(*cut)
    return gain


def bell_draw(rng, extent, spread, most, cuts=(), kind=jnp.bfloat16):
    result = jax.random.normal(rng, extent, jnp.float32) * spread
    if len(cuts) > 0:
        result = shard_levels(rng, extent, cuts, -0.22, 0.18) * result
    return jnp.clip(result, min=-most, max=most).astype(kind)


def setup_inputs(seed: int = 0) -> dict:
    arg_keys = jax.random.split(jax.random.key(seed), 11)
    return {
        "tokens": draw_tokens(jax.random.fold_in(arg_keys[10], 71), 0),
        "query_weight": bell_draw(arg_keys[1], (D, HEADS * HD), D ** -0.5, 0.09375, ((1, 4),)),
        "key_weight": bell_draw(arg_keys[2], (D, KV_HEADS * HD), D ** -0.5, 0.09375, ((1, 4),)),
        "value_weight": bell_draw(arg_keys[3], (D, KV_HEADS * HD), D ** -0.5, 0.09375, ((1, 4),)),
        "gate_weight": bell_draw(arg_keys[4], (D, 2 * HEADS), D ** -0.5, 0.09375),
        "summary_pos": bell_draw(arg_keys[5], (CMP, HD), 1.0, 6.0),
        "key_mixing": bell_draw(arg_keys[6], (CMP, KV_HEADS), CMP ** -0.5, 1.0),
        "value_mixing": bell_draw(arg_keys[7], (CMP, KV_HEADS), CMP ** -0.5, 1.0),
        "out_weight": bell_draw(arg_keys[8], (HEADS * HD, D), (HEADS * HD) ** -0.5, 0.125, ((0, 4),)),
        "chosen": draw_chosen(jax.random.fold_in(arg_keys[10], 71), 0),
    }


floor_score = -1e30


def masked_weights(scores, visible):
    probs = jax.nn.softmax(jnp.where(visible, scores, floor_score), axis=-1)
    return jnp.where(jnp.any(visible, axis=-1, keepdims=True), probs, 0.0)


def first_named(picked_ids):
    slot_count = picked_ids.shape[-1]
    repeated = picked_ids[..., :, None] == picked_ids[..., None, :]
    earlier = jnp.arange(slot_count)[None, :] < jnp.arange(slot_count)[:, None]
    return jnp.logical_not(jnp.any(repeated & earlier, axis=-1))


def summarize(source, offsets, mixing):
    span_count = source.shape[0] // CMP
    windows = source.astype(jnp.float32).reshape(span_count, CMP, source.shape[1], HD)
    windows = windows + offsets.astype(jnp.float32)[None, :, None, :]
    return jnp.einsum('njgd,jg->ngd', windows, mixing.astype(jnp.float32),
                      precision=lax.Precision.HIGHEST).astype(jnp.bfloat16)


def reference(tokens, query_weight, key_weight, value_weight, gate_weight, summary_pos, key_mixing,
              value_mixing, out_weight, chosen):
    length = tokens.shape[0]
    group_size = HEADS // KV_HEADS
    score_scale = HD ** -0.5
    queries = jnp.dot(tokens, query_weight, preferred_element_type=jnp.float32).astype(jnp.bfloat16)
    key_rows = jnp.dot(tokens, key_weight, preferred_element_type=jnp.float32).astype(jnp.bfloat16)
    key_rows = key_rows.reshape(length, KV_HEADS, HD)
    value_rows = jnp.dot(tokens, value_weight, preferred_element_type=jnp.float32).astype(jnp.bfloat16)
    value_rows = value_rows.reshape(length, KV_HEADS, HD)
    gate_vals = jax.nn.sigmoid(jnp.dot(tokens, gate_weight, preferred_element_type=jnp.float32))
    gate_vals = gate_vals.reshape(length // SB, SB, KV_HEADS, group_size, 2)
    key_summary = summarize(key_rows, summary_pos, key_mixing).astype(jnp.float32)
    value_summary = summarize(value_rows, summary_pos, value_mixing).astype(jnp.float32)
    span_ends = jnp.arange(length // CMP, dtype=jnp.int32) * CMP + (CMP - 1)
    block_table = jnp.concatenate([key_rows, value_rows], axis=-1).reshape(length // SB, SB, KV_HEADS, 2 * HD)
    head_ids = jnp.arange(KV_HEADS, dtype=jnp.int32)[:, None]
    unique_all = first_named(chosen)

    def one_block(inputs):
        query_blk, gate_blk, picked_ids, unique, offset = inputs
        query_pos = offset + jnp.arange(SB, dtype=jnp.int32)
        query_f = query_blk.astype(jnp.float32).reshape(SB, KV_HEADS, group_size, HD)
        summary_scores = jnp.einsum('qgrd,ngd->grqn', query_f, key_summary) * score_scale
        summary_probs = masked_weights(summary_scores, (span_ends[None, :] <= query_pos[:, None])[None, None])
        summary_probs = lax.optimization_barrier(summary_probs.astype(jnp.bfloat16)).astype(jnp.float32)
        summary_out = jnp.einsum('grqn,ngd->qgrd', summary_probs, value_summary)
        picked = block_table[picked_ids, :, head_ids, :]
        picked = picked.reshape(KV_HEADS, N_SEL * SB, 2 * HD).astype(jnp.float32)
        key_pos = (picked_ids[:, :, None] * SB + jnp.arange(SB, dtype=jnp.int32)).reshape(KV_HEADS, N_SEL * SB)
        counted = jnp.broadcast_to(unique[:, :, None], (KV_HEADS, N_SEL, SB)).reshape(KV_HEADS, N_SEL * SB)
        visible = counted[:, None, :] & (key_pos[:, None, :] <= query_pos[None, :, None])
        chosen_scores = jnp.einsum('qgrd,gmd->grqm', query_f, picked[..., :HD]) * score_scale
        chosen_probs = masked_weights(chosen_scores, visible[:, None])
        chosen_probs = lax.optimization_barrier(chosen_probs.astype(jnp.bfloat16)).astype(jnp.float32)
        chosen_out = jnp.einsum('grqm,gmd->qgrd', chosen_probs, picked[..., HD:])
        blended = gate_blk[..., 0:1] * summary_out + gate_blk[..., 1:2] * chosen_out
        return blended.reshape(SB, HEADS * HD).astype(jnp.bfloat16)

    offsets = jnp.arange(length // SB, dtype=jnp.int32) * SB
    attention = lax.map(one_block, (queries.reshape(length // SB, SB, HEADS * HD), gate_vals, chosen,
                                    unique_all, offsets)).reshape(length, HEADS * HD)
    width = HEADS * HD // N_TP
    summed = jnp.zeros((length, D), jnp.float32)
    for head_part in range(N_TP):
        partial_value = jnp.dot(attention[:, head_part * width:(head_part + 1) * width],
                          out_weight[head_part * width:(head_part + 1) * width],
                          preferred_element_type=jnp.float32).astype(jnp.bfloat16)
        summed = summed + lax.optimization_barrier(partial_value).astype(jnp.float32)
    return summed.astype(jnp.bfloat16)
```

```python
import functools

import jax
import jax.numpy as jnp
from jax import lax
from jax.experimental import pallas as pl
from jax.experimental.pallas import tpu as pltpu
from jax.sharding import PartitionSpec as P

HD = 64
CMP = 32
SB = 64
N_SEL = 16
LANES = 2 * HD
SPAN_PAD = 32
LOW = -1e30
FLOOR = -1e29
EXP_SCALE = HD ** (-0.5) * 1.4426950408889634
VMEM_LIMIT = 56 * 1024 * 1024


F32 = jnp.float32
BF16 = jnp.bfloat16


def lane_iota(rows):
    return lax.broadcasted_iota(jnp.int32, (rows, LANES), 1)


def row_iota(rows):
    return lax.broadcasted_iota(jnp.int32, (rows, LANES), 0)


def kv_kernel(part_ref, tok_ref, wk_ref, wv_ref, pos_ref, km_ref, vm_ref, kv_ref, sm_ref, acc_ref):
    step = pl.program_id(0)
    weight = jnp.concatenate([wk_ref[...], wv_ref[...]], axis=1)
    piece = jnp.dot(tok_ref[...], weight, preferred_element_type=F32)

    @pl.when(step == 0)
    def _():
        acc_ref[...] = piece

    @pl.when(step > 0)
    def _():
        acc_ref[...] += piece

    @pl.when(step == pl.num_programs(0) - 1)
    def _():
        heads, rows = kv_ref.shape[0], kv_ref.shape[1]
        spans = rows // CMP
        low_half = lane_iota(rows) < HD
        pos = pos_ref[...].astype(F32)
        pos = jnp.concatenate([pos, pos], axis=1)
        columns = lax.broadcasted_iota(jnp.int32, km_ref.shape, 1)
        for g in range(heads):
            pair = g // 2
            k = acc_ref[:, pair * LANES : (pair + 1) * LANES]
            v = acc_ref[:, (heads // 2 + pair) * LANES : (heads // 2 + pair + 1) * LANES]
            if g % 2 == 0:
                both = jnp.where(low_half, k, pltpu.roll(v, HD, 1))
            else:
                both = jnp.where(low_half, pltpu.roll(k, HD, 1), v)
            both = both.astype(BF16)
            kv_ref[g] = both
            mine = columns == part_ref[0] * heads + g
            kmix = jnp.sum(jnp.where(mine, km_ref[...].astype(F32), 0.0), axis=1, keepdims=True)
            vmix = jnp.sum(jnp.where(mine, vm_ref[...].astype(F32), 0.0), axis=1, keepdims=True)
            mix = jnp.where(lane_iota(CMP) < HD, kmix, vmix)
            windows = both.astype(F32).reshape(spans, CMP, LANES) + pos[None]
            total = jnp.sum(windows * mix[None], axis=1)
            pad = jnp.zeros((SPAN_PAD - spans, LANES), F32)
            sm_ref[g] = jnp.concatenate([total, pad], axis=0).astype(BF16)


def project_kv(part, tokens, key_weight, value_weight, pos, kmix, vmix):
    rows, depth = tokens.shape
    width = key_weight.shape[1]
    heads = width // HD
    chunk = depth // 4
    full = lambda shape: pl.BlockSpec(shape, lambda i, s: (0,) * len(shape))
    return pl.pallas_call(
        kv_kernel,
        grid_spec=pltpu.PrefetchScalarGridSpec(
            num_scalar_prefetch=1,
            grid=(depth // chunk,),
            in_specs=[
                pl.BlockSpec((rows, chunk), lambda i, s: (0, i)),
                pl.BlockSpec((chunk, width), lambda i, s: (i, 0)),
                pl.BlockSpec((chunk, width), lambda i, s: (i, 0)),
                full(pos.shape),
                full(kmix.shape),
                full(vmix.shape),
            ],
            out_specs=[full((heads, rows, LANES)), full((heads, SPAN_PAD, LANES))],
            scratch_shapes=[pltpu.VMEM((rows, 2 * width), F32)],
        ),
        out_shape=[
            jax.ShapeDtypeStruct((heads, rows, LANES), BF16),
            jax.ShapeDtypeStruct((heads, SPAN_PAD, LANES), BF16),
        ],
        cost_estimate=pl.CostEstimate(
            flops=4 * rows * depth * width, transcendentals=0, bytes_accessed=2 * depth * (rows + 2 * width)
        ),
        compiler_params=pltpu.CompilerParams(vmem_limit_bytes=VMEM_LIMIT),
        name="kv_proj",
    )(part, tokens, key_weight, value_weight, pos, kmix, vmix)


def q_kernel(part_ref, tok_ref, wq_ref, gw_ref, q_ref, gate_ref, acc_ref, gacc_ref):
    step = pl.program_id(0)
    gates = gate_ref.shape[1]
    start = pl.multiple_of(part_ref[0] * gates, gates)
    gate_rows = gw_ref[pl.ds(start, gates), :]
    piece = jnp.dot(tok_ref[...], wq_ref[...], preferred_element_type=F32)
    gpiece = lax.dot_general(tok_ref[...], gate_rows, (((1,), (1,)), ((), ())), preferred_element_type=F32)

    @pl.when(step == 0)
    def _():
        acc_ref[...] = piece
        gacc_ref[...] = gpiece

    @pl.when(step > 0)
    def _():
        acc_ref[...] += piece
        gacc_ref[...] += gpiece

    @pl.when(step == pl.num_programs(0) - 1)
    def _():
        heads, rows = q_ref.shape[0], q_ref.shape[1]
        lane, inner = lane_iota(rows), lax.rem(row_iota(rows), SB)
        low_half = lane < HD
        ext = jnp.where((lane == HD) | (lane - HD > inner), 1.0, 0.0)
        for h in range(heads):
            slab = acc_ref[:, (h // 2) * LANES : (h // 2 + 1) * LANES]
            if h % 2:
                slab = pltpu.roll(slab, HD, 1)
            q_ref[h] = jnp.where(low_half, slab, ext).astype(BF16)
        gate_ref[...] = jax.nn.sigmoid(gacc_ref[...])


def project_q(part, tokens, query_weight, gate_rows):
    rows, depth = tokens.shape
    width = query_weight.shape[1]
    heads = width // HD
    chunk = depth // 4
    return pl.pallas_call(
        q_kernel,
        grid_spec=pltpu.PrefetchScalarGridSpec(
            num_scalar_prefetch=1,
            grid=(depth // chunk,),
            in_specs=[
                pl.BlockSpec((rows, chunk), lambda i, s: (0, i)),
                pl.BlockSpec((chunk, width), lambda i, s: (i, 0)),
                pl.BlockSpec((gate_rows.shape[0], chunk), lambda i, s: (0, i)),
            ],
            out_specs=[
                pl.BlockSpec((heads, rows, LANES), lambda i, s: (0, 0, 0)),
                pl.BlockSpec((rows, 2 * heads), lambda i, s: (0, 0)),
            ],
            scratch_shapes=[pltpu.VMEM((rows, width), F32), pltpu.VMEM((rows, 2 * heads), F32)],
        ),
        out_shape=[
            jax.ShapeDtypeStruct((heads, rows, LANES), BF16),
            jax.ShapeDtypeStruct((rows, 2 * heads), F32),
        ],
        cost_estimate=pl.CostEstimate(
            flops=3 * rows * depth * width, transcendentals=0, bytes_accessed=2 * depth * (rows + width)
        ),
        compiler_params=pltpu.CompilerParams(vmem_limit_bytes=VMEM_LIMIT),
        name="q_proj",
    )(part, tokens, query_weight, gate_rows)


def select_kernel(count, own_ref, req_ref, kv_ref, sm_ref, *out_refs):
    heads = kv_ref.shape[0]
    own = own_ref[0]
    for shift in range(1, count):
        taker = jnp.minimum(own + shift, count - 1)
        out_ref = out_refs[shift - 1]
        for g in range(heads):
            for j in range(2):
                block = req_ref[taker, own * (2 * heads) + 2 * g + j]
                out_ref[g, j * SB : (j + 1) * SB, :] = kv_ref[g, pl.ds(pl.multiple_of(block * SB, SB), SB), :]
            out_ref[g, 2 * SB :, :] = sm_ref[g]


def select_blocks(count, own, requests, kv, summaries):
    heads = kv.shape[0]
    piece = (heads, 2 * SB + SPAN_PAD, LANES)
    vmem = pl.BlockSpec(memory_space=pltpu.VMEM)
    smem = pl.BlockSpec(memory_space=pltpu.SMEM)
    return pl.pallas_call(
        functools.partial(select_kernel, count),
        in_specs=[smem, smem, vmem, vmem],
        out_specs=[vmem] * (count - 1),
        out_shape=[jax.ShapeDtypeStruct(piece, BF16)] * (count - 1),
        compiler_params=pltpu.CompilerParams(vmem_limit_bytes=VMEM_LIMIT),
        name="select_blocks",
    )(own, requests, kv, summaries)


def attn_kernel(count, *refs):
    base_ref, own_ref, table_ref, q_ref, gate_ref, kv_ref, sm_ref = refs[:7]
    recv_refs = refs[7 : 7 + count - 1]
    out_ref, poolk, poolv, sumk, sumv, kbuf, vbuf = refs[7 + count - 1 :]
    step = pl.program_id(0)
    own = own_ref[0]
    block = base_ref[0] + step
    heads, rows = kv_ref.shape[0], kv_ref.shape[1]
    group = q_ref.shape[0] // heads
    own_blocks = rows // SB
    spans = rows // CMP
    total_blocks = poolk.shape[1] - 1
    lane, row = lane_iota(SB), row_iota(SB)
    keep = jnp.where(lane < HD, 1.0, 0.0).astype(BF16)
    other = jnp.where(lane < HD, 0.0, 1.0).astype(BF16)
    span_lane, span_row = lane_iota(SPAN_PAD), row_iota(SPAN_PAD)

    @pl.when(step == 0)
    def _():
        for g in range(heads):
            for j in range(own_blocks):
                piece = kv_ref[g, j * SB : (j + 1) * SB, :]
                poolk[g, j] = piece * keep
                poolv[g, j] = piece * other + keep
            for k, recv in enumerate(recv_refs):
                for j in range(2):
                    piece = recv[g, j * SB : (j + 1) * SB, :]
                    poolk[g, own_blocks + 2 * k + j] = piece * keep
                    poolv[g, own_blocks + 2 * k + j] = piece * other + keep
            poolk[g, total_blocks] = jnp.where(lane == HD, LOW, 0.0).astype(BF16)
            poolv[g, total_blocks] = jnp.zeros((SB, LANES), BF16)
            for k in range(count):
                piece = sm_ref[g] if k == 0 else recv_refs[k - 1][g, 2 * SB :, :]
                sumv[g, k * SPAN_PAD : (k + 1) * SPAN_PAD] = piece * other[:SPAN_PAD] + keep[:SPAN_PAD]
                if k:
                    hidden = (span_lane == HD) & ((span_row >= spans) | (own < k))
                    bias = jnp.where(hidden, LOW, 0.0).astype(BF16)
                    sumk[g, k * SPAN_PAD : (k + 1) * SPAN_PAD] = piece * keep[:SPAN_PAD] + bias

    diagonal = jnp.where((lane - HD == row) & (row > 0), LOW, 0.0).astype(BF16)
    last = SB // CMP * block
    hidden = (span_lane == HD) & (span_row >= last + SB // CMP)
    for j in range(SB // CMP):
        hidden = hidden | ((span_row == last + j) & (span_lane == HD + (j + 1) * CMP - 1))
    bias = jnp.where(hidden, LOW, 0.0).astype(BF16)
    contract = (((1,), (1,)), ((), ()))
    low_half = lane < HD
    for g in range(heads):
        for s in range(N_SEL):
            place = table_ref[block, g * N_SEL + s]
            piece = poolk[g, place]
            if s == 0:
                piece = piece + diagonal
            kbuf[g, s * SB : (s + 1) * SB, :] = piece
            vbuf[g, s * SB : (s + 1) * SB, :] = poolv[g, place]
        sumk[g, 0:SPAN_PAD] = sm_ref[g] * keep[:SPAN_PAD] + bias
        q = q_ref[g * group : (g + 1) * group].reshape(group * SB, LANES)
        score = lax.dot_general(q, kbuf[g], contract, preferred_element_type=F32)
        top = jnp.max(score, axis=1, keepdims=True)
        weight = jnp.exp2((score - top) * EXP_SCALE).astype(BF16)
        picked = jnp.dot(weight, vbuf[g], preferred_element_type=F32)
        score = lax.dot_general(q, sumk[g], contract, preferred_element_type=F32)
        top = jnp.maximum(jnp.max(score, axis=1, keepdims=True), FLOOR)
        weight = jnp.exp2((score - top) * EXP_SCALE).astype(BF16)
        summed = jnp.dot(weight, sumv[g], preferred_element_type=F32)
        for pair in range(group // 2):
            mixed = []
            for r in (2 * pair, 2 * pair + 1):
                h = g * group + r
                a = summed[r * SB : (r + 1) * SB]
                c = picked[r * SB : (r + 1) * SB]
                ca = gate_ref[:, 2 * h : 2 * h + 1] / jnp.maximum(a, 1e-30)
                cc = gate_ref[:, 2 * h + 1 : 2 * h + 2] / c
                if r % 2 == 0:
                    mixed.append(pltpu.roll(a, HD, 1) * ca + pltpu.roll(c, HD, 1) * cc)
                else:
                    mixed.append(a * pltpu.roll(ca, HD, 1) + c * pltpu.roll(cc, HD, 1))
            both = jnp.where(low_half, mixed[0], mixed[1]).astype(BF16)
            at = (g * group) // 2 + pair
            out_ref[:, at * LANES : (at + 1) * LANES] = both


def attend(count, blocks, base, own, table, q, gates, kv, summaries, received):
    heads, rows = kv.shape[0], kv.shape[1]
    total = rows // SB + 2 * (count - 1)
    full = lambda shape: pl.BlockSpec(shape, lambda i, *s: (0,) * len(shape))
    return pl.pallas_call(
        functools.partial(attn_kernel, count),
        grid_spec=pltpu.PrefetchScalarGridSpec(
            num_scalar_prefetch=3,
            grid=(blocks,),
            in_specs=[
                pl.BlockSpec((q.shape[0], SB, LANES), lambda i, base, *s: (0, base[0] + i, 0)),
                pl.BlockSpec((SB, gates.shape[1]), lambda i, base, *s: (base[0] + i, 0)),
                full(kv.shape),
                full(summaries.shape),
                *[full(r.shape) for r in received],
            ],
            out_specs=pl.BlockSpec((SB, q.shape[0] * HD), lambda i, *s: (i, 0)),
            scratch_shapes=[
                pltpu.VMEM((heads, total + 1, SB, LANES), BF16),
                pltpu.VMEM((heads, total + 1, SB, LANES), BF16),
                pltpu.VMEM((heads, count * SPAN_PAD, LANES), BF16),
                pltpu.VMEM((heads, count * SPAN_PAD, LANES), BF16),
                pltpu.VMEM((heads, N_SEL * SB, LANES), BF16),
                pltpu.VMEM((heads, N_SEL * SB, LANES), BF16),
            ],
        ),
        out_shape=jax.ShapeDtypeStruct((blocks * SB, q.shape[0] * HD), BF16),
        cost_estimate=pl.CostEstimate(
            flops=blocks * q.shape[0] * SB * (N_SEL * SB + count * SPAN_PAD) * LANES * 4,
            transcendentals=blocks * q.shape[0] * SB * N_SEL * SB,
            bytes_accessed=4 * kv.size,
        ),
        compiler_params=pltpu.CompilerParams(vmem_limit_bytes=VMEM_LIMIT),
        name="attend",
    )(base, own, table, q, gates, kv, summaries, *received)


def local(count, parts, tokens, query_weight, key_weight, value_weight, gate_weight, summary_pos, key_mixing,
          value_mixing, out_weight, chosen):
    rows = tokens.shape[0]
    own = lax.axis_index("kv").astype(jnp.int32)
    part = lax.axis_index("tp").astype(jnp.int32)
    own_blocks = rows // SB
    heads = key_weight.shape[1] // HD
    own1, part1 = own.reshape(1), part.reshape(1)

    source = chosen // own_blocks
    place = chosen - source * own_blocks
    match = source[None] == jnp.arange(count, dtype=jnp.int32)[:, None, None, None]
    lowest = jnp.min(jnp.where(match, place[None], own_blocks - 1), axis=(1, 3))
    highest = jnp.max(jnp.where(match, place[None], 0), axis=(1, 3))
    request = jnp.stack([lowest, highest], axis=-1).reshape(1, count * heads * 2)
    everyone = jnp.where(jnp.arange(count, dtype=jnp.int32)[:, None] == own, request, 0)
    if count & (count - 1) == 0:
        bit = 1
        while bit < count:
            everyone = everyone + lax.ppermute(everyone, "kv", [(i, i ^ bit) for i in range(count)])
            bit *= 2
    else:
        everyone = lax.all_gather(request, "kv", axis=0, tiled=True)

    kv, summaries = project_kv(part1, tokens, key_weight, value_weight, summary_pos, key_mixing, value_mixing)
    q, gates = project_q(part1, tokens, query_weight, gate_weight.T)

    pieces = select_blocks(count, own1, everyone, kv, summaries)
    received = [
        lax.ppermute(pieces[k - 1], "kv", [(i, i + k) for i in range(count - k)]) for k in range(1, count)
    ]

    high_at = jnp.sum(jnp.where(match, highest[:, None, :, None], 0), axis=0)
    away = own_blocks + 2 * (own - source - 1) + (place == high_at).astype(jnp.int32)
    index = jnp.where(source == own, place, away)
    slots = jnp.arange(N_SEL, dtype=jnp.int32)
    earlier = slots[None, :] < slots[:, None]
    repeated = jnp.any((chosen[..., :, None] == chosen[..., None, :]) & earlier, axis=-1)
    first = jnp.logical_not(repeated)
    rank = jnp.sum((first[..., None, :] & earlier).astype(jnp.int32), axis=-1)
    at = (rank[..., None, :] == slots[:, None]) & first[..., None, :]
    fill = own_blocks + 2 * (count - 1)
    table = jnp.where(jnp.any(at, axis=-1), jnp.sum(jnp.where(at, index[..., None, :], 0), axis=-1), fill)
    table = table.reshape(own_blocks, heads * N_SEL)

    half_blocks = own_blocks // 2
    half = part // 2
    core = part % 2
    third = rows // parts

    def halves(which):
        return attend(count, half_blocks, (which * half_blocks).reshape(1), own1, table, q, gates, kv, summaries,
                      received)

    def product(att, columns):
        return jnp.dot(att, columns, preferred_element_type=F32).astype(BF16)

    def rows_of(att, which):
        return lax.dynamic_slice_in_dim(att, which * third, third, 0)

    swap = [(i, i ^ 1) for i in range(parts)]
    cross = [(i, i ^ 2) for i in range(parts)]
    chunks = 4
    width = out_weight.shape[1] // chunks
    far = halves(1 - half)
    far_keep, far_send = rows_of(far, core), rows_of(far, 1 - core)
    crossed = []
    for c in range(chunks):
        columns = out_weight[:, c * width : (c + 1) * width]
        got = lax.ppermute(product(far_send, columns), "tp", swap)
        kept = product(far_keep, columns)
        both = (got.astype(F32) + kept.astype(F32)).astype(BF16)
        crossed.append(lax.ppermute(both, "tp", cross))
    near = halves(half)
    got = lax.ppermute(product(rows_of(near, 1 - core), out_weight), "tp", swap)
    kept = product(rows_of(near, core), out_weight)
    base = got.astype(F32) + kept.astype(F32)
    return jnp.concatenate(
        [
            (base[:, c * width : (c + 1) * width] + crossed[c].astype(F32)).astype(BF16)
            for c in range(chunks)
        ],
        axis=1,
    )


def solution(mesh):
    placed = (
        P("kv", None),
        P(None, "tp"),
        P(None, "tp"),
        P(None, "tp"),
        P(),
        P(),
        P(),
        P(),
        P("tp", None),
        P("kv", "tp", None),
    )
    body = functools.partial(local, mesh.shape["kv"], mesh.shape["tp"])
    return jax.shard_map(
        body, mesh=mesh, in_specs=placed, out_specs=P(("kv", "tp"), None), check_vma=False
    )
```

```python
import functools

import jax
import jax.numpy as jnp
from jax import lax
from jax.experimental import pallas as pl
from jax.experimental.pallas import tpu as pltpu
from jax.sharding import PartitionSpec as P


HD = 64
CMP = 32
SB = 64
N_SEL = 16
LANES = 2 * HD
SPAN_PAD = 32
CHUNKS = 4
LOW = -1e30
FLOOR = -1e29
EXP_SCALE = HD ** (-0.5) * 1.4426950408889634
VMEM_LIMIT = 56 * 1024 * 1024


F32 = jnp.float32
BF16 = jnp.bfloat16


def lane_iota(rows):
    return lax.broadcasted_iota(jnp.int32, (rows, LANES), 1)


def row_iota(rows):
    return lax.broadcasted_iota(jnp.int32, (rows, LANES), 0)


def kv_kernel(part_ref, tok_ref, wk_ref, wv_ref, pos_ref, km_ref, vm_ref, kv_ref, sm_ref, acc_ref):
    step = pl.program_id(0)
    weight = jnp.concatenate([wk_ref[...], wv_ref[...]], axis=1)
    piece = jnp.dot(tok_ref[...], weight, preferred_element_type=F32)

    @pl.when(step == 0)
    def _():
        acc_ref[...] = piece

    @pl.when(step > 0)
    def _():
        acc_ref[...] += piece

    @pl.when(step == pl.num_programs(0) - 1)
    def _():
        heads, rows = kv_ref.shape[0], kv_ref.shape[1]
        spans = rows // CMP
        low_half = lane_iota(rows) < HD
        pos = pos_ref[...].astype(F32)
        pos = jnp.concatenate([pos, pos], axis=1)
        columns = lax.broadcasted_iota(jnp.int32, km_ref.shape, 1)
        for g in range(heads):
            pair = g // 2
            k = acc_ref[:, pair * LANES : (pair + 1) * LANES]
            v = acc_ref[:, (heads // 2 + pair) * LANES : (heads // 2 + pair + 1) * LANES]
            if g % 2 == 0:
                both = jnp.where(low_half, k, pltpu.roll(v, HD, 1))
            else:
                both = jnp.where(low_half, pltpu.roll(k, HD, 1), v)
            both = both.astype(BF16)
            kv_ref[g] = both
            mine = columns == part_ref[0] * heads + g
            kmix = jnp.sum(jnp.where(mine, km_ref[...].astype(F32), 0.0), axis=1, keepdims=True)
            vmix = jnp.sum(jnp.where(mine, vm_ref[...].astype(F32), 0.0), axis=1, keepdims=True)
            mix = jnp.where(lane_iota(CMP) < HD, kmix, vmix)
            windows = both.astype(F32).reshape(spans, CMP, LANES) + pos[None]
            total = jnp.sum(windows * mix[None], axis=1)
            pad = jnp.zeros((SPAN_PAD - spans, LANES), F32)
            sm_ref[g] = jnp.concatenate([total, pad], axis=0).astype(BF16)


def project_kv(part, tokens, key_weight, value_weight, pos, kmix, vmix):
    rows, depth = tokens.shape
    width = key_weight.shape[1]
    heads = width // HD
    chunk = depth // 4
    full = lambda shape: pl.BlockSpec(shape, lambda i, s: (0,) * len(shape))
    return pl.pallas_call(
        kv_kernel,
        grid_spec=pltpu.PrefetchScalarGridSpec(
            num_scalar_prefetch=1,
            grid=(depth // chunk,),
            in_specs=[
                pl.BlockSpec((rows, chunk), lambda i, s: (0, i)),
                pl.BlockSpec((chunk, width), lambda i, s: (i, 0)),
                pl.BlockSpec((chunk, width), lambda i, s: (i, 0)),
                full(pos.shape),
                full(kmix.shape),
                full(vmix.shape),
            ],
            out_specs=[full((heads, rows, LANES)), full((heads, SPAN_PAD, LANES))],
            scratch_shapes=[pltpu.VMEM((rows, 2 * width), F32)],
        ),
        out_shape=[
            jax.ShapeDtypeStruct((heads, rows, LANES), BF16),
            jax.ShapeDtypeStruct((heads, SPAN_PAD, LANES), BF16),
        ],
        cost_estimate=pl.CostEstimate(
            flops=4 * rows * depth * width, transcendentals=0, bytes_accessed=2 * depth * (rows + 2 * width)
        ),
        compiler_params=pltpu.CompilerParams(vmem_limit_bytes=VMEM_LIMIT),
        name="kv_proj",
    )(part, tokens, key_weight, value_weight, pos, kmix, vmix)


def q_kernel(part_ref, tok_ref, wq_ref, gw_ref, q_ref, gate_ref, acc_ref, gacc_ref):
    step = pl.program_id(0)
    gates = gate_ref.shape[1]
    start = pl.multiple_of(part_ref[0] * gates, gates)
    gate_rows = gw_ref[pl.ds(start, gates), :]
    piece = jnp.dot(tok_ref[...], wq_ref[...], preferred_element_type=F32)
    gpiece = lax.dot_general(tok_ref[...], gate_rows, (((1,), (1,)), ((), ())), preferred_element_type=F32)

    @pl.when(step == 0)
    def _():
        acc_ref[...] = piece
        gacc_ref[...] = gpiece

    @pl.when(step > 0)
    def _():
        acc_ref[...] += piece
        gacc_ref[...] += gpiece

    @pl.when(step == pl.num_programs(0) - 1)
    def _():
        heads, rows = q_ref.shape[0], q_ref.shape[1]
        lane, inner = lane_iota(rows), lax.rem(row_iota(rows), SB)
        low_half = lane < HD
        ext = jnp.where((lane == HD) | (lane - HD > inner), 1.0, 0.0)
        for h in range(heads):
            slab = acc_ref[:, (h // 2) * LANES : (h // 2 + 1) * LANES]
            if h % 2:
                slab = pltpu.roll(slab, HD, 1)
            q_ref[h] = jnp.where(low_half, slab, ext).astype(BF16)
        gate_ref[...] = jax.nn.sigmoid(gacc_ref[...])


def project_q(part, tokens, query_weight, gate_rows):
    rows, depth = tokens.shape
    width = query_weight.shape[1]
    heads = width // HD
    chunk = depth // 4
    return pl.pallas_call(
        q_kernel,
        grid_spec=pltpu.PrefetchScalarGridSpec(
            num_scalar_prefetch=1,
            grid=(depth // chunk,),
            in_specs=[
                pl.BlockSpec((rows, chunk), lambda i, s: (0, i)),
                pl.BlockSpec((chunk, width), lambda i, s: (i, 0)),
                pl.BlockSpec((gate_rows.shape[0], chunk), lambda i, s: (0, i)),
            ],
            out_specs=[
                pl.BlockSpec((heads, rows, LANES), lambda i, s: (0, 0, 0)),
                pl.BlockSpec((rows, 2 * heads), lambda i, s: (0, 0)),
            ],
            scratch_shapes=[pltpu.VMEM((rows, width), F32), pltpu.VMEM((rows, 2 * heads), F32)],
        ),
        out_shape=[
            jax.ShapeDtypeStruct((heads, rows, LANES), BF16),
            jax.ShapeDtypeStruct((rows, 2 * heads), F32),
        ],
        cost_estimate=pl.CostEstimate(
            flops=3 * rows * depth * width, transcendentals=0, bytes_accessed=2 * depth * (rows + width)
        ),
        compiler_params=pltpu.CompilerParams(vmem_limit_bytes=VMEM_LIMIT),
        name="q_proj",
    )(part, tokens, query_weight, gate_rows)


def select_kernel(count, own_ref, req_ref, kv_ref, sm_ref, *out_refs):
    heads = kv_ref.shape[0]
    own = own_ref[0]
    for shift in range(1, count):
        taker = jnp.minimum(own + shift, count - 1)
        out_ref = out_refs[shift - 1]
        for g in range(heads):
            for j in range(2):
                block = req_ref[taker, own * (2 * heads) + 2 * g + j]
                out_ref[g, j * SB : (j + 1) * SB, :] = kv_ref[g, pl.ds(pl.multiple_of(block * SB, SB), SB), :]
            out_ref[g, 2 * SB :, :] = sm_ref[g]


def select_blocks(count, own, requests, kv, summaries):
    heads = kv.shape[0]
    piece = (heads, 2 * SB + SPAN_PAD, LANES)
    vmem = pl.BlockSpec(memory_space=pltpu.VMEM)
    smem = pl.BlockSpec(memory_space=pltpu.SMEM)
    return pl.pallas_call(
        functools.partial(select_kernel, count),
        in_specs=[smem, smem, vmem, vmem],
        out_specs=[vmem] * (count - 1),
        out_shape=[jax.ShapeDtypeStruct(piece, BF16)] * (count - 1),
        compiler_params=pltpu.CompilerParams(vmem_limit_bytes=VMEM_LIMIT),
        name="select_blocks",
    )(own, requests, kv, summaries)


def attn_kernel(count, *refs):
    base_ref, own_ref, table_ref, q_ref, gate_ref, kv_ref, sm_ref = refs[:7]
    recv_refs = refs[7 : 7 + count - 1]
    out_ref, poolk, poolv, sumk, sumv, kbuf, vbuf = refs[7 + count - 1 :]
    step = pl.program_id(0)
    own = own_ref[0]
    block = base_ref[0] + step
    heads, rows = kv_ref.shape[0], kv_ref.shape[1]
    group = q_ref.shape[0] // heads
    own_blocks = rows // SB
    spans = rows // CMP
    total_blocks = poolk.shape[1] - 1
    lane, row = lane_iota(SB), row_iota(SB)
    keep = jnp.where(lane < HD, 1.0, 0.0).astype(BF16)
    other = jnp.where(lane < HD, 0.0, 1.0).astype(BF16)
    span_lane, span_row = lane_iota(SPAN_PAD), row_iota(SPAN_PAD)

    @pl.when(step == 0)
    def _():
        for g in range(heads):
            for j in range(own_blocks):
                piece = kv_ref[g, j * SB : (j + 1) * SB, :]
                poolk[g, j] = piece * keep
                poolv[g, j] = piece * other + keep
            for k, recv in enumerate(recv_refs):
                for j in range(2):
                    piece = recv[g, j * SB : (j + 1) * SB, :]
                    poolk[g, own_blocks + 2 * k + j] = piece * keep
                    poolv[g, own_blocks + 2 * k + j] = piece * other + keep
            poolk[g, total_blocks] = jnp.where(lane == HD, LOW, 0.0).astype(BF16)
            poolv[g, total_blocks] = jnp.zeros((SB, LANES), BF16)
            for k in range(count):
                piece = sm_ref[g] if k == 0 else recv_refs[k - 1][g, 2 * SB :, :]
                sumv[g, k * SPAN_PAD : (k + 1) * SPAN_PAD] = piece * other[:SPAN_PAD] + keep[:SPAN_PAD]
                if k:
                    hidden = (span_lane == HD) & ((span_row >= spans) | (own < k))
                    bias = jnp.where(hidden, LOW, 0.0).astype(BF16)
                    sumk[g, k * SPAN_PAD : (k + 1) * SPAN_PAD] = piece * keep[:SPAN_PAD] + bias

    diagonal = jnp.where((lane - HD == row) & (row > 0), LOW, 0.0).astype(BF16)
    last = SB // CMP * block
    hidden = (span_lane == HD) & (span_row >= last + SB // CMP)
    for j in range(SB // CMP):
        hidden = hidden | ((span_row == last + j) & (span_lane == HD + (j + 1) * CMP - 1))
    bias = jnp.where(hidden, LOW, 0.0).astype(BF16)
    contract = (((1,), (1,)), ((), ()))
    low_half = lane < HD
    for g in range(heads):
        for s in range(N_SEL):
            place = table_ref[block, g * N_SEL + s]
            piece = poolk[g, place]
            if s == 0:
                piece = piece + diagonal
            kbuf[g, s * SB : (s + 1) * SB, :] = piece
            vbuf[g, s * SB : (s + 1) * SB, :] = poolv[g, place]
        sumk[g, 0:SPAN_PAD] = sm_ref[g] * keep[:SPAN_PAD] + bias
        q = q_ref[g * group : (g + 1) * group].reshape(group * SB, LANES)
        score = lax.dot_general(q, kbuf[g], contract, preferred_element_type=F32)
        top = jnp.max(score, axis=1, keepdims=True)
        weight = jnp.exp2((score - top) * EXP_SCALE).astype(BF16)
        picked = jnp.dot(weight, vbuf[g], preferred_element_type=F32)
        score = lax.dot_general(q, sumk[g], contract, preferred_element_type=F32)
        top = jnp.maximum(jnp.max(score, axis=1, keepdims=True), FLOOR)
        weight = jnp.exp2((score - top) * EXP_SCALE).astype(BF16)
        summed = jnp.dot(weight, sumv[g], preferred_element_type=F32)
        for pair in range(group // 2):
            mixed = []
            for r in (2 * pair, 2 * pair + 1):
                h = g * group + r
                a = summed[r * SB : (r + 1) * SB]
                c = picked[r * SB : (r + 1) * SB]
                ca = gate_ref[:, 2 * h : 2 * h + 1] / jnp.maximum(a, 1e-30)
                cc = gate_ref[:, 2 * h + 1 : 2 * h + 2] / c
                if r % 2 == 0:
                    mixed.append(pltpu.roll(a, HD, 1) * ca + pltpu.roll(c, HD, 1) * cc)
                else:
                    mixed.append(a * pltpu.roll(ca, HD, 1) + c * pltpu.roll(cc, HD, 1))
            both = jnp.where(low_half, mixed[0], mixed[1]).astype(BF16)
            at = (g * group) // 2 + pair
            out_ref[:, at * LANES : (at + 1) * LANES] = both


def attend(count, blocks, base, own, table, q, gates, kv, summaries, received):
    heads, rows = kv.shape[0], kv.shape[1]
    total = rows // SB + 2 * (count - 1)
    full = lambda shape: pl.BlockSpec(shape, lambda i, *s: (0,) * len(shape))
    return pl.pallas_call(
        functools.partial(attn_kernel, count),
        grid_spec=pltpu.PrefetchScalarGridSpec(
            num_scalar_prefetch=3,
            grid=(blocks,),
            in_specs=[
                pl.BlockSpec((q.shape[0], SB, LANES), lambda i, base, *s: (0, base[0] + i, 0)),
                pl.BlockSpec((SB, gates.shape[1]), lambda i, base, *s: (base[0] + i, 0)),
                full(kv.shape),
                full(summaries.shape),
                *[full(r.shape) for r in received],
            ],
            out_specs=pl.BlockSpec((SB, q.shape[0] * HD), lambda i, *s: (i, 0)),
            scratch_shapes=[
                pltpu.VMEM((heads, total + 1, SB, LANES), BF16),
                pltpu.VMEM((heads, total + 1, SB, LANES), BF16),
                pltpu.VMEM((heads, count * SPAN_PAD, LANES), BF16),
                pltpu.VMEM((heads, count * SPAN_PAD, LANES), BF16),
                pltpu.VMEM((heads, N_SEL * SB, LANES), BF16),
                pltpu.VMEM((heads, N_SEL * SB, LANES), BF16),
            ],
        ),
        out_shape=jax.ShapeDtypeStruct((blocks * SB, q.shape[0] * HD), BF16),
        cost_estimate=pl.CostEstimate(
            flops=blocks * q.shape[0] * SB * (N_SEL * SB + count * SPAN_PAD) * LANES * 4,
            transcendentals=blocks * q.shape[0] * SB * N_SEL * SB,
            bytes_accessed=4 * kv.size,
        ),
        compiler_params=pltpu.CompilerParams(vmem_limit_bytes=VMEM_LIMIT),
        name="attend",
    )(base, own, table, q, gates, kv, summaries, *received)


def local(count, parts, tokens, query_weight, key_weight, value_weight, gate_weight, summary_pos, key_mixing,
          value_mixing, out_weight, chosen):
    rows = tokens.shape[0]
    own = lax.axis_index("kv").astype(jnp.int32)
    part = lax.axis_index("tp").astype(jnp.int32)
    own_blocks = rows // SB
    heads = key_weight.shape[1] // HD
    own1, part1 = own.reshape(1), part.reshape(1)

    source = chosen // own_blocks
    place = chosen - source * own_blocks
    match = source[None] == jnp.arange(count, dtype=jnp.int32)[:, None, None, None]
    lowest = jnp.min(jnp.where(match, place[None], own_blocks - 1), axis=(1, 3))
    highest = jnp.max(jnp.where(match, place[None], 0), axis=(1, 3))
    request = jnp.stack([lowest, highest], axis=-1).reshape(1, count * heads * 2)
    everyone = jnp.where(jnp.arange(count, dtype=jnp.int32)[:, None] == own, request, 0)
    if count & (count - 1) == 0:
        bit, stage = 1, 0
        while bit < count:
            got = lax.ppermute(everyone, "kv", [(i, i ^ bit) for i in range(count)])
            everyone = everyone + got
            if stage == 0:
                chosen = lax.optimization_barrier((chosen, got))[0]
            bit, stage = 2 * bit, stage + 1
    else:
        everyone = lax.all_gather(request, "kv", axis=0, tiled=True)

    kv, summaries = project_kv(part1, tokens, key_weight, value_weight, summary_pos, key_mixing, value_mixing)
    q, gates = project_q(part1, tokens, query_weight, gate_weight.T)

    pieces = select_blocks(count, own1, everyone, kv, summaries)
    received = []
    for k in range(1, count):
        received.append(lax.ppermute(pieces[k - 1], "kv", [(i, i + k) for i in range(count - k)]))

    source = chosen // own_blocks
    place = chosen - source * own_blocks
    match = source[None] == jnp.arange(count, dtype=jnp.int32)[:, None, None, None]

    high_at = jnp.sum(jnp.where(match, highest[:, None, :, None], 0), axis=0)
    away = own_blocks + 2 * (own - source - 1) + (place == high_at).astype(jnp.int32)
    index = jnp.where(source == own, place, away)
    slots = jnp.arange(N_SEL, dtype=jnp.int32)
    earlier = slots[None, :] < slots[:, None]
    repeated = jnp.any((chosen[..., :, None] == chosen[..., None, :]) & earlier, axis=-1)
    first = jnp.logical_not(repeated)
    rank = jnp.sum((first[..., None, :] & earlier).astype(jnp.int32), axis=-1)
    at = (rank[..., None, :] == slots[:, None]) & first[..., None, :]
    fill = own_blocks + 2 * (count - 1)
    table = jnp.where(jnp.any(at, axis=-1), jnp.sum(jnp.where(at, index[..., None, :], 0), axis=-1), fill)
    table = table.reshape(own_blocks, heads * N_SEL)

    half_blocks = own_blocks // 2
    half = part // 2
    core = part % 2
    third = rows // parts

    def halves(which):
        return attend(count, half_blocks, (which * half_blocks).reshape(1), own1, table, q, gates, kv, summaries,
                      received)

    def product(att, columns):
        return jnp.dot(att, columns, preferred_element_type=F32).astype(BF16)

    def rows_of(att, which):
        return lax.dynamic_slice_in_dim(att, which * third, third, 0)

    swap = [(i, i ^ 1) for i in range(parts)]
    cross = [(i, i ^ 2) for i in range(parts)]
    width = out_weight.shape[1] // CHUNKS
    far = halves(1 - half)
    far_keep, far_send = rows_of(far, core), rows_of(far, 1 - core)
    crossed = []
    for c in range(CHUNKS):
        columns = out_weight[:, c * width : (c + 1) * width]
        piece = product(far_send, columns)
        got = lax.ppermute(piece, "tp", swap)
        kept = product(far_keep, columns)
        both = (got.astype(F32) + kept.astype(F32)).astype(BF16)
        crossed.append(lax.ppermute(both, "tp", cross))
    near = halves(half)
    got = lax.ppermute(product(rows_of(near, 1 - core), out_weight), "tp", swap)
    kept = product(rows_of(near, core), out_weight)
    base = got.astype(F32) + kept.astype(F32)
    return jnp.concatenate(
        [
            (base[:, c * width : (c + 1) * width] + crossed[c].astype(F32)).astype(BF16)
            for c in range(CHUNKS)
        ],
        axis=1,
    )


def solution(mesh):
    placed = (
        P("kv", None),
        P(None, "tp"),
        P(None, "tp"),
        P(None, "tp"),
        P(),
        P(),
        P(),
        P(),
        P("tp", None),
        P("kv", "tp", None),
    )
    count = mesh.shape["kv"]

    def body(*args):
        return local(count, mesh.shape["tp"], *args)

    return jax.shard_map(
        body, mesh=mesh, in_specs=placed, out_specs=P(("kv", "tp"), None), check_vma=False
    )
```

```python
import functools

import jax
import jax.numpy as jnp
from jax import lax
from jax.experimental import pallas as pl
from jax.experimental.pallas import tpu as pltpu
from jax.sharding import PartitionSpec as P


HD = 64
CMP = 32
SB = 64
N_SEL = 16
LANES = 2 * HD
SPAN_PAD = 32
CHUNKS = 4
LOW = -1e30
FLOOR = -1e29
EXP_SCALE = HD ** (-0.5) * 1.4426950408889634
VMEM_LIMIT = 56 * 1024 * 1024


F32 = jnp.float32
BF16 = jnp.bfloat16


def lane_iota(rows):
    return lax.broadcasted_iota(jnp.int32, (rows, LANES), 1)


def row_iota(rows):
    return lax.broadcasted_iota(jnp.int32, (rows, LANES), 0)


def proj_kernel(part_ref, tok_ref, wq_ref, wk_ref, wv_ref, gw_ref, pos_ref, km_ref, vm_ref, q_ref, gate_ref, kv_ref,
                sm_ref, acc_ref, gacc_ref):
    step = pl.program_id(0)
    gates = gate_ref.shape[1]
    start = pl.multiple_of(part_ref[0] * gates, gates)
    weight = jnp.concatenate([wq_ref[...], wk_ref[...], wv_ref[...]], axis=1)
    piece = jnp.dot(tok_ref[...], weight, preferred_element_type=F32)
    gpiece = lax.dot_general(
        tok_ref[...], gw_ref[pl.ds(start, gates), :], (((1,), (1,)), ((), ())), preferred_element_type=F32
    )

    @pl.when(step == 0)
    def _():
        acc_ref[...] = piece
        gacc_ref[...] = gpiece

    @pl.when(step > 0)
    def _():
        acc_ref[...] += piece
        gacc_ref[...] += gpiece

    @pl.when(step == pl.num_programs(0) - 1)
    def _():
        heads, rows = q_ref.shape[0], q_ref.shape[1]
        key_heads = kv_ref.shape[0]
        lane, inner = lane_iota(rows), lax.rem(row_iota(rows), SB)
        low_half = lane < HD
        ext = jnp.where((lane == HD) | (lane - HD > inner), 1.0, 0.0)
        for h in range(heads):
            slab = acc_ref[:, (h // 2) * LANES : (h // 2 + 1) * LANES]
            if h % 2:
                slab = pltpu.roll(slab, HD, 1)
            q_ref[h] = jnp.where(low_half, slab, ext).astype(BF16)
        gate_ref[...] = jax.nn.sigmoid(gacc_ref[...])

        spans = rows // CMP
        pos = pos_ref[...].astype(F32)
        pos = jnp.concatenate([pos, pos], axis=1)
        line = lax.broadcasted_iota(jnp.int32, km_ref.shape, 0)
        eye = lax.broadcasted_iota(jnp.int32, (CMP, CMP), 0) == lax.broadcasted_iota(jnp.int32, (CMP, CMP), 1)

        def column(ref, head):
            kept = jnp.sum(jnp.where(line == head, ref[...].astype(F32), 0.0), axis=0, keepdims=True)
            return jnp.sum(jnp.where(eye, kept, 0.0), axis=1, keepdims=True)

        at_k, at_v = heads * HD, heads * HD + key_heads * HD
        for g in range(key_heads):
            k = acc_ref[:, at_k + (g // 2) * LANES : at_k + (g // 2 + 1) * LANES]
            v = acc_ref[:, at_v + (g // 2) * LANES : at_v + (g // 2 + 1) * LANES]
            if g % 2 == 0:
                both = jnp.where(low_half, k, pltpu.roll(v, HD, 1))
            else:
                both = jnp.where(low_half, pltpu.roll(k, HD, 1), v)
            both = both.astype(BF16)
            kv_ref[g] = both
            head = part_ref[0] * key_heads + g
            mix = jnp.where(lane_iota(CMP) < HD, column(km_ref, head), column(vm_ref, head))
            windows = both.astype(F32).reshape(spans, CMP, LANES) + pos[None]
            total = jnp.sum(windows * mix[None], axis=1)
            pad = jnp.zeros((SPAN_PAD - spans, LANES), F32)
            sm_ref[g] = jnp.concatenate([total, pad], axis=0).astype(BF16)


def project(part, tokens, query_weight, key_weight, value_weight, gate_rows, pos, kmix, vmix):
    rows, depth = tokens.shape
    qwidth, width = query_weight.shape[1], key_weight.shape[1]
    heads, key_heads = qwidth // HD, width // HD
    chunk = depth // 4
    full = lambda shape: pl.BlockSpec(shape, lambda i, s: (0,) * len(shape))
    return pl.pallas_call(
        proj_kernel,
        grid_spec=pltpu.PrefetchScalarGridSpec(
            num_scalar_prefetch=1,
            grid=(depth // chunk,),
            in_specs=[
                pl.BlockSpec((rows, chunk), lambda i, s: (0, i)),
                pl.BlockSpec((chunk, qwidth), lambda i, s: (i, 0)),
                pl.BlockSpec((chunk, width), lambda i, s: (i, 0)),
                pl.BlockSpec((chunk, width), lambda i, s: (i, 0)),
                pl.BlockSpec((gate_rows.shape[0], chunk), lambda i, s: (0, i)),
                full(pos.shape),
                full(kmix.shape),
                full(vmix.shape),
            ],
            out_specs=[
                full((heads, rows, LANES)),
                full((rows, 2 * heads)),
                full((key_heads, rows, LANES)),
                full((key_heads, SPAN_PAD, LANES)),
            ],
            scratch_shapes=[pltpu.VMEM((rows, qwidth + 2 * width), F32), pltpu.VMEM((rows, 2 * heads), F32)],
        ),
        out_shape=[
            jax.ShapeDtypeStruct((heads, rows, LANES), BF16),
            jax.ShapeDtypeStruct((rows, 2 * heads), F32),
            jax.ShapeDtypeStruct((key_heads, rows, LANES), BF16),
            jax.ShapeDtypeStruct((key_heads, SPAN_PAD, LANES), BF16),
        ],
        cost_estimate=pl.CostEstimate(
            flops=2 * rows * depth * (qwidth + 3 * width), transcendentals=0, bytes_accessed=2 * depth * (rows + qwidth)
        ),
        compiler_params=pltpu.CompilerParams(vmem_limit_bytes=VMEM_LIMIT),
        name="project",
    )(part, tokens, query_weight, key_weight, value_weight, gate_rows, pos, kmix, vmix)


def select_kernel(count, own_ref, req_ref, kv_ref, sm_ref, *out_refs):
    heads = kv_ref.shape[0]
    own = own_ref[0]
    for shift in range(1, count):
        taker = jnp.minimum(own + shift, count - 1)
        out_ref = out_refs[shift - 1]
        for g in range(heads):
            for j in range(2):
                block = req_ref[taker, own * (2 * heads) + 2 * g + j]
                out_ref[g, j * SB : (j + 1) * SB, :] = kv_ref[g, pl.ds(pl.multiple_of(block * SB, SB), SB), :]
            out_ref[g, 2 * SB :, :] = sm_ref[g]


def select_blocks(count, own, requests, kv, summaries):
    heads = kv.shape[0]
    piece = (heads, 2 * SB + SPAN_PAD, LANES)
    vmem = pl.BlockSpec(memory_space=pltpu.VMEM)
    smem = pl.BlockSpec(memory_space=pltpu.SMEM)
    return pl.pallas_call(
        functools.partial(select_kernel, count),
        in_specs=[smem, smem, vmem, vmem],
        out_specs=[vmem] * (count - 1),
        out_shape=[jax.ShapeDtypeStruct(piece, BF16)] * (count - 1),
        compiler_params=pltpu.CompilerParams(vmem_limit_bytes=VMEM_LIMIT),
        name="select_blocks",
    )(own, requests, kv, summaries)


def attn_kernel(count, *refs):
    base_ref, own_ref, table_ref, q_ref, gate_ref, kv_ref, sm_ref = refs[:7]
    recv_refs = refs[7 : 7 + count - 1]
    out_ref, poolk, poolv, sumk, sumv, kbuf, vbuf = refs[7 + count - 1 :]
    step = pl.program_id(0)
    own = own_ref[0]
    block = base_ref[0] + step
    heads, rows = kv_ref.shape[0], kv_ref.shape[1]
    group = q_ref.shape[0] // heads
    own_blocks = rows // SB
    spans = rows // CMP
    total_blocks = poolk.shape[1] - 1
    lane, row = lane_iota(SB), row_iota(SB)
    keep = jnp.where(lane < HD, 1.0, 0.0).astype(BF16)
    other = jnp.where(lane < HD, 0.0, 1.0).astype(BF16)
    span_lane, span_row = lane_iota(SPAN_PAD), row_iota(SPAN_PAD)

    @pl.when(step == 0)
    def _():
        for g in range(heads):
            for j in range(own_blocks):
                piece = kv_ref[g, j * SB : (j + 1) * SB, :]
                poolk[g, j] = piece * keep
                poolv[g, j] = piece * other + keep
            for k, recv in enumerate(recv_refs):
                for j in range(2):
                    piece = recv[g, j * SB : (j + 1) * SB, :]
                    poolk[g, own_blocks + 2 * k + j] = piece * keep
                    poolv[g, own_blocks + 2 * k + j] = piece * other + keep
            poolk[g, total_blocks] = jnp.where(lane == HD, LOW, 0.0).astype(BF16)
            poolv[g, total_blocks] = jnp.zeros((SB, LANES), BF16)
            for k in range(count):
                piece = sm_ref[g] if k == 0 else recv_refs[k - 1][g, 2 * SB :, :]
                sumv[g, k * SPAN_PAD : (k + 1) * SPAN_PAD] = piece * other[:SPAN_PAD] + keep[:SPAN_PAD]
                if k:
                    hidden = (span_lane == HD) & ((span_row >= spans) | (own < k))
                    bias = jnp.where(hidden, LOW, 0.0).astype(BF16)
                    sumk[g, k * SPAN_PAD : (k + 1) * SPAN_PAD] = piece * keep[:SPAN_PAD] + bias

    diagonal = jnp.where((lane - HD == row) & (row > 0), LOW, 0.0).astype(BF16)
    last = SB // CMP * block
    hidden = (span_lane == HD) & (span_row >= last + SB // CMP)
    for j in range(SB // CMP):
        hidden = hidden | ((span_row == last + j) & (span_lane == HD + (j + 1) * CMP - 1))
    bias = jnp.where(hidden, LOW, 0.0).astype(BF16)
    contract = (((1,), (1,)), ((), ()))
    low_half = lane < HD
    for g in range(heads):
        for s in range(N_SEL):
            place = table_ref[block, g * N_SEL + s]
            piece = poolk[g, place]
            if s == 0:
                piece = piece + diagonal
            kbuf[g, s * SB : (s + 1) * SB, :] = piece
            vbuf[g, s * SB : (s + 1) * SB, :] = poolv[g, place]
        sumk[g, 0:SPAN_PAD] = sm_ref[g] * keep[:SPAN_PAD] + bias
        q = q_ref[g * group : (g + 1) * group].reshape(group * SB, LANES)
        score = lax.dot_general(q, kbuf[g], contract, preferred_element_type=F32)
        top = jnp.max(score, axis=1, keepdims=True)
        weight = jnp.exp2((score - top) * EXP_SCALE).astype(BF16)
        picked = jnp.dot(weight, vbuf[g], preferred_element_type=F32)
        score = lax.dot_general(q, sumk[g], contract, preferred_element_type=F32)
        top = jnp.maximum(jnp.max(score, axis=1, keepdims=True), FLOOR)
        weight = jnp.exp2((score - top) * EXP_SCALE).astype(BF16)
        summed = jnp.dot(weight, sumv[g], preferred_element_type=F32)
        for pair in range(group // 2):
            mixed = []
            for r in (2 * pair, 2 * pair + 1):
                h = g * group + r
                a = summed[r * SB : (r + 1) * SB]
                c = picked[r * SB : (r + 1) * SB]
                ca = gate_ref[:, 2 * h : 2 * h + 1] / jnp.maximum(a, 1e-30)
                cc = gate_ref[:, 2 * h + 1 : 2 * h + 2] / c
                if r % 2 == 0:
                    mixed.append(pltpu.roll(a, HD, 1) * ca + pltpu.roll(c, HD, 1) * cc)
                else:
                    mixed.append(a * pltpu.roll(ca, HD, 1) + c * pltpu.roll(cc, HD, 1))
            both = jnp.where(low_half, mixed[0], mixed[1]).astype(BF16)
            at = (g * group) // 2 + pair
            out_ref[:, at * LANES : (at + 1) * LANES] = both


def attend(count, blocks, base, own, table, q, gates, kv, summaries, received):
    heads, rows = kv.shape[0], kv.shape[1]
    total = rows // SB + 2 * (count - 1)
    full = lambda shape: pl.BlockSpec(shape, lambda i, *s: (0,) * len(shape))
    return pl.pallas_call(
        functools.partial(attn_kernel, count),
        grid_spec=pltpu.PrefetchScalarGridSpec(
            num_scalar_prefetch=3,
            grid=(blocks,),
            in_specs=[
                pl.BlockSpec((q.shape[0], SB, LANES), lambda i, base, *s: (0, base[0] + i, 0)),
                pl.BlockSpec((SB, gates.shape[1]), lambda i, base, *s: (base[0] + i, 0)),
                full(kv.shape),
                full(summaries.shape),
                *[full(r.shape) for r in received],
            ],
            out_specs=pl.BlockSpec((SB, q.shape[0] * HD), lambda i, *s: (i, 0)),
            scratch_shapes=[
                pltpu.VMEM((heads, total + 1, SB, LANES), BF16),
                pltpu.VMEM((heads, total + 1, SB, LANES), BF16),
                pltpu.VMEM((heads, count * SPAN_PAD, LANES), BF16),
                pltpu.VMEM((heads, count * SPAN_PAD, LANES), BF16),
                pltpu.VMEM((heads, N_SEL * SB, LANES), BF16),
                pltpu.VMEM((heads, N_SEL * SB, LANES), BF16),
            ],
        ),
        out_shape=jax.ShapeDtypeStruct((blocks * SB, q.shape[0] * HD), BF16),
        cost_estimate=pl.CostEstimate(
            flops=blocks * q.shape[0] * SB * (N_SEL * SB + count * SPAN_PAD) * LANES * 4,
            transcendentals=blocks * q.shape[0] * SB * N_SEL * SB,
            bytes_accessed=4 * kv.size,
        ),
        compiler_params=pltpu.CompilerParams(vmem_limit_bytes=VMEM_LIMIT),
        name="attend",
    )(base, own, table, q, gates, kv, summaries, *received)


def local(count, parts, tokens, query_weight, key_weight, value_weight, gate_weight, summary_pos, key_mixing,
          value_mixing, out_weight, chosen):
    rows = tokens.shape[0]
    own = lax.axis_index("kv").astype(jnp.int32)
    part = lax.axis_index("tp").astype(jnp.int32)
    own_blocks = rows // SB
    heads = key_weight.shape[1] // HD
    own1, part1 = own.reshape(1), part.reshape(1)

    source = chosen // own_blocks
    place = chosen - source * own_blocks
    match = source[None] == jnp.arange(count, dtype=jnp.int32)[:, None, None, None]
    lowest = jnp.min(jnp.where(match, place[None], own_blocks - 1), axis=(1, 3))
    highest = jnp.max(jnp.where(match, place[None], 0), axis=(1, 3))
    request = jnp.stack([lowest, highest], axis=-1).reshape(1, count * heads * 2)
    everyone = jnp.where(jnp.arange(count, dtype=jnp.int32)[:, None] == own, request, 0)
    if count & (count - 1) == 0:
        bit, stage = 1, 0
        while bit < count:
            got = lax.ppermute(everyone, "kv", [(i, i ^ bit) for i in range(count)])
            everyone = everyone + got
            if stage == 0:
                chosen = lax.optimization_barrier((chosen, got))[0]
            bit, stage = 2 * bit, stage + 1
    else:
        everyone = lax.all_gather(request, "kv", axis=0, tiled=True)

    q, gates, kv, summaries = project(
        part1, tokens, query_weight, key_weight, value_weight, gate_weight.T, summary_pos, key_mixing.T,
        value_mixing.T,
    )

    pieces = select_blocks(count, own1, everyone, kv, summaries)
    received = []
    for k in range(1, count):
        received.append(lax.ppermute(pieces[k - 1], "kv", [(i, i + k) for i in range(count - k)]))

    source = chosen // own_blocks
    place = chosen - source * own_blocks
    match = source[None] == jnp.arange(count, dtype=jnp.int32)[:, None, None, None]

    high_at = jnp.sum(jnp.where(match, highest[:, None, :, None], 0), axis=0)
    away = own_blocks + 2 * (own - source - 1) + (place == high_at).astype(jnp.int32)
    index = jnp.where(source == own, place, away)
    slots = jnp.arange(N_SEL, dtype=jnp.int32)
    earlier = slots[None, :] < slots[:, None]
    repeated = jnp.any((chosen[..., :, None] == chosen[..., None, :]) & earlier, axis=-1)
    first = jnp.logical_not(repeated)
    rank = jnp.sum((first[..., None, :] & earlier).astype(jnp.int32), axis=-1)
    at = (rank[..., None, :] == slots[:, None]) & first[..., None, :]
    fill = own_blocks + 2 * (count - 1)
    table = jnp.where(jnp.any(at, axis=-1), jnp.sum(jnp.where(at, index[..., None, :], 0), axis=-1), fill)
    table = table.reshape(own_blocks, heads * N_SEL)

    half_blocks = own_blocks // 2
    half = part // 2
    core = part % 2
    third = rows // parts

    def halves(which):
        return attend(count, half_blocks, (which * half_blocks).reshape(1), own1, table, q, gates, kv, summaries,
                      received)

    def product(att, columns):
        return jnp.dot(att, columns, preferred_element_type=F32).astype(BF16)

    def rows_of(att, which):
        return lax.dynamic_slice_in_dim(att, which * third, third, 0)

    swap = [(i, i ^ 1) for i in range(parts)]
    cross = [(i, i ^ 2) for i in range(parts)]
    width = out_weight.shape[1] // CHUNKS
    far = halves(1 - half)
    far_keep, far_send = rows_of(far, core), rows_of(far, 1 - core)
    crossed = []
    for c in range(CHUNKS):
        columns = out_weight[:, c * width : (c + 1) * width]
        piece = product(far_send, columns)
        got = lax.ppermute(piece, "tp", swap)
        kept = product(far_keep, columns)
        both = (got.astype(F32) + kept.astype(F32)).astype(BF16)
        crossed.append(lax.ppermute(both, "tp", cross))
    near = halves(half)
    got = lax.ppermute(product(rows_of(near, 1 - core), out_weight), "tp", swap)
    kept = product(rows_of(near, core), out_weight)
    base = got.astype(F32) + kept.astype(F32)
    return jnp.concatenate(
        [
            (base[:, c * width : (c + 1) * width] + crossed[c].astype(F32)).astype(BF16)
            for c in range(CHUNKS)
        ],
        axis=1,
    )


def solution(mesh):
    placed = (
        P("kv", None),
        P(None, "tp"),
        P(None, "tp"),
        P(None, "tp"),
        P(),
        P(),
        P(),
        P(),
        P("tp", None),
        P("kv", "tp", None),
    )
    count = mesh.shape["kv"]

    def body(*args):
        return local(count, mesh.shape["tp"], *args)

    return jax.shard_map(
        body, mesh=mesh, in_specs=placed, out_specs=P(("kv", "tp"), None), check_vma=False
    )
```

```python
import functools

import jax
import jax.numpy as jnp
from jax import lax
from jax.experimental import pallas as pl
from jax.experimental.pallas import tpu as pltpu
from jax.sharding import PartitionSpec as P


HD = 64
CMP = 32
SB = 64
N_SEL = 16
LANES = 2 * HD
SPAN_PAD = 32
SLOT_STEPS = (8, 12)
LOW = -1e30
FLOOR = -1e29
EXP_SCALE = HD ** (-0.5) * 1.4426950408889634
VMEM_LIMIT = 56 * 1024 * 1024


F32 = jnp.float32
BF16 = jnp.bfloat16


def lane_iota(rows):
    return lax.broadcasted_iota(jnp.int32, (rows, LANES), 1)


def row_iota(rows):
    return lax.broadcasted_iota(jnp.int32, (rows, LANES), 0)


def proj_kernel(part_ref, tok_ref, wq_ref, wk_ref, wv_ref, gw_ref, pos_ref, km_ref, vm_ref, q_ref, gate_ref, kv_ref,
                sm_ref, acc_ref, gacc_ref):
    step = pl.program_id(0)
    gates = gate_ref.shape[1]
    start = pl.multiple_of(part_ref[0] * gates, gates)
    weight = jnp.concatenate([wq_ref[...], wk_ref[...], wv_ref[...]], axis=1)
    piece = jnp.dot(tok_ref[...], weight, preferred_element_type=F32)
    gpiece = lax.dot_general(
        tok_ref[...], gw_ref[pl.ds(start, gates), :], (((1,), (1,)), ((), ())), preferred_element_type=F32
    )

    @pl.when(step == 0)
    def _():
        acc_ref[...] = piece
        gacc_ref[...] = gpiece

    @pl.when(step > 0)
    def _():
        acc_ref[...] += piece
        gacc_ref[...] += gpiece

    @pl.when(step == pl.num_programs(0) - 1)
    def _():
        heads, rows = q_ref.shape[0], q_ref.shape[1]
        key_heads = kv_ref.shape[0]
        lane, inner = lane_iota(rows), lax.rem(row_iota(rows), SB)
        low_half = lane < HD
        ext = jnp.where((lane == HD) | (lane - HD > inner), 1.0, 0.0)
        for h in range(heads):
            slab = acc_ref[:, (h // 2) * LANES : (h // 2 + 1) * LANES]
            if h % 2:
                slab = pltpu.roll(slab, HD, 1)
            q_ref[h] = jnp.where(low_half, slab, ext).astype(BF16)
        gate_ref[...] = jax.nn.sigmoid(gacc_ref[...])

        spans = rows // CMP
        pos = pos_ref[...].astype(F32)
        pos = jnp.concatenate([pos, pos], axis=1)
        line = lax.broadcasted_iota(jnp.int32, km_ref.shape, 0)
        eye = lax.broadcasted_iota(jnp.int32, (CMP, CMP), 0) == lax.broadcasted_iota(jnp.int32, (CMP, CMP), 1)

        def column(ref, head):
            kept = jnp.sum(jnp.where(line == head, ref[...].astype(F32), 0.0), axis=0, keepdims=True)
            return jnp.sum(jnp.where(eye, kept, 0.0), axis=1, keepdims=True)

        at_k, at_v = heads * HD, heads * HD + key_heads * HD
        for g in range(key_heads):
            k = acc_ref[:, at_k + (g // 2) * LANES : at_k + (g // 2 + 1) * LANES]
            v = acc_ref[:, at_v + (g // 2) * LANES : at_v + (g // 2 + 1) * LANES]
            if g % 2 == 0:
                both = jnp.where(low_half, k, pltpu.roll(v, HD, 1))
            else:
                both = jnp.where(low_half, pltpu.roll(k, HD, 1), v)
            both = both.astype(BF16)
            kv_ref[g] = both
            head = part_ref[0] * key_heads + g
            mix = jnp.where(lane_iota(CMP) < HD, column(km_ref, head), column(vm_ref, head))
            windows = both.astype(F32).reshape(spans, CMP, LANES) + pos[None]
            total = jnp.sum(windows * mix[None], axis=1)
            pad = jnp.zeros((SPAN_PAD - spans, LANES), F32)
            sm_ref[g] = jnp.concatenate([total, pad], axis=0).astype(BF16)


def project(part, tokens, query_weight, key_weight, value_weight, gate_rows, pos, kmix, vmix):
    rows, depth = tokens.shape
    qwidth, width = query_weight.shape[1], key_weight.shape[1]
    heads, key_heads = qwidth // HD, width // HD
    chunk = depth // 4
    full = lambda shape: pl.BlockSpec(shape, lambda i, s: (0,) * len(shape))
    return pl.pallas_call(
        proj_kernel,
        grid_spec=pltpu.PrefetchScalarGridSpec(
            num_scalar_prefetch=1,
            grid=(depth // chunk,),
            in_specs=[
                pl.BlockSpec((rows, chunk), lambda i, s: (0, i)),
                pl.BlockSpec((chunk, qwidth), lambda i, s: (i, 0)),
                pl.BlockSpec((chunk, width), lambda i, s: (i, 0)),
                pl.BlockSpec((chunk, width), lambda i, s: (i, 0)),
                pl.BlockSpec((gate_rows.shape[0], chunk), lambda i, s: (0, i)),
                full(pos.shape),
                full(kmix.shape),
                full(vmix.shape),
            ],
            out_specs=[
                full((heads, rows, LANES)),
                full((rows, 2 * heads)),
                full((key_heads, rows, LANES)),
                full((key_heads, SPAN_PAD, LANES)),
            ],
            scratch_shapes=[pltpu.VMEM((rows, qwidth + 2 * width), F32), pltpu.VMEM((rows, 2 * heads), F32)],
        ),
        out_shape=[
            jax.ShapeDtypeStruct((heads, rows, LANES), BF16),
            jax.ShapeDtypeStruct((rows, 2 * heads), F32),
            jax.ShapeDtypeStruct((key_heads, rows, LANES), BF16),
            jax.ShapeDtypeStruct((key_heads, SPAN_PAD, LANES), BF16),
        ],
        cost_estimate=pl.CostEstimate(
            flops=2 * rows * depth * (qwidth + 3 * width), transcendentals=0, bytes_accessed=2 * depth * (rows + qwidth)
        ),
        compiler_params=pltpu.CompilerParams(vmem_limit_bytes=VMEM_LIMIT),
        name="project",
    )(part, tokens, query_weight, key_weight, value_weight, gate_rows, pos, kmix, vmix)


def select_kernel(count, own_ref, req_ref, kv_ref, sm_ref, *out_refs):
    heads = kv_ref.shape[0]
    own = own_ref[0]
    for shift in range(1, count):
        taker = jnp.minimum(own + shift, count - 1)
        out_ref = out_refs[shift - 1]
        for g in range(heads):
            for j in range(2):
                block = req_ref[taker, own * (2 * heads) + 2 * g + j]
                out_ref[g, j * SB : (j + 1) * SB, :] = kv_ref[g, pl.ds(pl.multiple_of(block * SB, SB), SB), :]
            out_ref[g, 2 * SB :, :] = sm_ref[g]


def select_blocks(count, own, requests, kv, summaries):
    heads = kv.shape[0]
    piece = (heads, 2 * SB + SPAN_PAD, LANES)
    vmem = pl.BlockSpec(memory_space=pltpu.VMEM)
    smem = pl.BlockSpec(memory_space=pltpu.SMEM)
    return pl.pallas_call(
        functools.partial(select_kernel, count),
        in_specs=[smem, smem, vmem, vmem],
        out_specs=[vmem] * (count - 1),
        out_shape=[jax.ShapeDtypeStruct(piece, BF16)] * (count - 1),
        compiler_params=pltpu.CompilerParams(vmem_limit_bytes=VMEM_LIMIT),
        name="select_blocks",
    )(own, requests, kv, summaries)


def attn_kernel(count, *refs):
    base_ref, own_ref, table_ref, q_ref, gate_ref, kv_ref, sm_ref = refs[:7]
    recv_refs = refs[7 : 7 + count - 1]
    out_ref, poolk, pool, sumk, sumv, kbuf, vbuf = refs[7 + count - 1 :]
    step = pl.program_id(0)
    own = own_ref[0]
    block = base_ref[0] + step
    heads, rows = kv_ref.shape[0], kv_ref.shape[1]
    group = q_ref.shape[0] // heads
    own_blocks = rows // SB
    spans = rows // CMP
    total_blocks = poolk.shape[1] - 1
    lane, row = lane_iota(SB), row_iota(SB)
    keep = jnp.where(lane < HD, 1.0, 0.0).astype(BF16)
    other = jnp.where(lane < HD, 0.0, 1.0).astype(BF16)
    span_lane, span_row = lane_iota(SPAN_PAD), row_iota(SPAN_PAD)

    @pl.when(step == 0)
    def _():
        for g in range(heads):
            for j in range(own_blocks):
                piece = kv_ref[g, j * SB : (j + 1) * SB, :]
                pool[g, j] = piece
                poolk[g, j] = piece * keep
            for k, recv in enumerate(recv_refs):
                for j in range(2):
                    piece = recv[g, j * SB : (j + 1) * SB, :]
                    pool[g, own_blocks + 2 * k + j] = piece
                    poolk[g, own_blocks + 2 * k + j] = piece * keep
            pool[g, total_blocks] = jnp.zeros((SB, LANES), BF16)
            poolk[g, total_blocks] = jnp.where(lane == HD, LOW, 0.0).astype(BF16)
            for k in range(count):
                piece = sm_ref[g] if k == 0 else recv_refs[k - 1][g, 2 * SB :, :]
                sumv[g, k * SPAN_PAD : (k + 1) * SPAN_PAD] = piece * other[:SPAN_PAD] + keep[:SPAN_PAD]
                if k:
                    hidden = (span_lane == HD) & ((span_row >= spans) | (own < k))
                    bias = jnp.where(hidden, LOW, 0.0).astype(BF16)
                    sumk[g, k * SPAN_PAD : (k + 1) * SPAN_PAD] = piece * keep[:SPAN_PAD] + bias

    diagonal = jnp.where((lane - HD == row) & (row > 0), LOW, 0.0).astype(BF16)
    last = SB // CMP * block
    hidden = (span_lane == HD) & (span_row >= last + SB // CMP)
    for j in range(SB // CMP):
        hidden = hidden | ((span_row == last + j) & (span_lane == HD + (j + 1) * CMP - 1))
    bias = jnp.where(hidden, LOW, 0.0).astype(BF16)
    contract = (((1,), (1,)), ((), ()))
    low_half = lane < HD
    for g in range(heads):
        sumk[g, 0:SPAN_PAD] = sm_ref[g] * keep[:SPAN_PAD] + bias

    def one(slots):
        for g in range(heads):
            for s in range(slots):
                place = table_ref[block, g * N_SEL + s]
                piece = pool[g, place]
                if s == 0:
                    kbuf[g, s * SB : (s + 1) * SB, :] = piece * keep + diagonal
                else:
                    kbuf[g, s * SB : (s + 1) * SB, :] = poolk[g, place]
                vbuf[g, s * SB : (s + 1) * SB, :] = piece * other + keep
            q = q_ref[g * group : (g + 1) * group].reshape(group * SB, LANES)
            score = lax.dot_general(q, kbuf[g, : slots * SB], contract, preferred_element_type=F32)
            top = jnp.max(score, axis=1, keepdims=True)
            weight = jnp.exp2((score - top) * EXP_SCALE).astype(BF16)
            picked = jnp.dot(weight, vbuf[g, : slots * SB], preferred_element_type=F32)
            score = lax.dot_general(q, sumk[g], contract, preferred_element_type=F32)
            top = jnp.maximum(jnp.max(score, axis=1, keepdims=True), FLOOR)
            weight = jnp.exp2((score - top) * EXP_SCALE).astype(BF16)
            summed = jnp.dot(weight, sumv[g], preferred_element_type=F32)
            for pair in range(group // 2):
                mixed = []
                for r in (2 * pair, 2 * pair + 1):
                    h = g * group + r
                    a = summed[r * SB : (r + 1) * SB]
                    c = picked[r * SB : (r + 1) * SB]
                    ca = gate_ref[:, 2 * h : 2 * h + 1] / jnp.maximum(a, 1e-30)
                    cc = gate_ref[:, 2 * h + 1 : 2 * h + 2] / c
                    if r % 2 == 0:
                        mixed.append(pltpu.roll(a, HD, 1) * ca + pltpu.roll(c, HD, 1) * cc)
                    else:
                        mixed.append(a * pltpu.roll(ca, HD, 1) + c * pltpu.roll(cc, HD, 1))
                both = jnp.where(low_half, mixed[0], mixed[1]).astype(BF16)
                at = (g * group) // 2 + pair
                out_ref[:, at * LANES : (at + 1) * LANES] = both

    def past(slots):
        named = [table_ref[block, g * N_SEL + slots] != total_blocks for g in range(heads)]
        return functools.reduce(jnp.logical_or, named)

    sizes = [slots for slots in SLOT_STEPS if slots < N_SEL] + [N_SEL]
    for k, slots in enumerate(sizes):
        taken = past(sizes[k - 1]) if k else None
        if slots < N_SEL:
            short = jnp.logical_not(past(slots))
            taken = short if taken is None else jnp.logical_and(taken, short)
        pl.when(taken)(functools.partial(one, slots))


def attend(count, blocks, base, own, table, q, gates, kv, summaries, received):
    heads, rows = kv.shape[0], kv.shape[1]
    total = rows // SB + 2 * (count - 1)
    return pl.pallas_call(
        functools.partial(attn_kernel, count),
        grid_spec=pltpu.PrefetchScalarGridSpec(
            num_scalar_prefetch=3,
            grid=(blocks,),
            in_specs=[
                pl.BlockSpec((q.shape[0], SB, LANES), lambda i, base, *s: (0, base[0] + i, 0)),
                pl.BlockSpec((SB, gates.shape[1]), lambda i, base, *s: (base[0] + i, 0)),
                *[pl.BlockSpec(memory_space=pltpu.VMEM)] * (2 + len(received)),
            ],
            out_specs=pl.BlockSpec((SB, q.shape[0] * HD), lambda i, *s: (i, 0)),
            scratch_shapes=[
                pltpu.VMEM((heads, total + 1, SB, LANES), BF16),
                pltpu.VMEM((heads, total + 1, SB, LANES), BF16),
                pltpu.VMEM((heads, count * SPAN_PAD, LANES), BF16),
                pltpu.VMEM((heads, count * SPAN_PAD, LANES), BF16),
                pltpu.VMEM((heads, N_SEL * SB, LANES), BF16),
                pltpu.VMEM((heads, N_SEL * SB, LANES), BF16),
            ],
        ),
        out_shape=jax.ShapeDtypeStruct((blocks * SB, q.shape[0] * HD), BF16),
        cost_estimate=pl.CostEstimate(
            flops=blocks * q.shape[0] * SB * (N_SEL * SB + count * SPAN_PAD) * LANES * 4,
            transcendentals=blocks * q.shape[0] * SB * N_SEL * SB,
            bytes_accessed=4 * kv.size,
        ),
        compiler_params=pltpu.CompilerParams(vmem_limit_bytes=VMEM_LIMIT),
        name="attend",
    )(base, own, table, q, gates, kv, summaries, *received)


def local(count, parts, tokens, query_weight, key_weight, value_weight, gate_weight, summary_pos, key_mixing,
          value_mixing, out_weight, chosen):
    rows = tokens.shape[0]
    own = lax.axis_index("kv").astype(jnp.int32)
    part = lax.axis_index("tp").astype(jnp.int32)
    own_blocks = rows // SB
    heads = key_weight.shape[1] // HD
    own1, part1 = own.reshape(1), part.reshape(1)

    source = chosen // own_blocks
    place = chosen - source * own_blocks
    match = source[None] == jnp.arange(count, dtype=jnp.int32)[:, None, None, None]
    lowest = jnp.min(jnp.where(match, place[None], own_blocks - 1), axis=(1, 3))
    highest = jnp.max(jnp.where(match, place[None], 0), axis=(1, 3))
    request = jnp.stack([lowest, highest], axis=-1).reshape(1, count * heads * 2)
    everyone = jnp.where(jnp.arange(count, dtype=jnp.int32)[:, None] == own, request, 0)
    if count & (count - 1) == 0:
        bit, stage = 1, 0
        while bit < count:
            got = lax.ppermute(everyone, "kv", [(i, i ^ bit) for i in range(count)])
            everyone = everyone + got
            if stage == 0:
                chosen = lax.optimization_barrier((chosen, got))[0]
            bit, stage = 2 * bit, stage + 1
    else:
        everyone = lax.all_gather(request, "kv", axis=0, tiled=True)

    q, gates, kv, summaries = project(
        part1, tokens, query_weight, key_weight, value_weight, gate_weight.T, summary_pos, key_mixing.T,
        value_mixing.T,
    )

    pieces = select_blocks(count, own1, everyone, kv, summaries)
    received = []
    for k in range(1, count):
        received.append(lax.ppermute(pieces[k - 1], "kv", [(i, i + k) for i in range(count - k)]))

    source = chosen // own_blocks
    place = chosen - source * own_blocks
    match = source[None] == jnp.arange(count, dtype=jnp.int32)[:, None, None, None]

    high_at = jnp.sum(jnp.where(match, highest[:, None, :, None], 0), axis=0)
    away = own_blocks + 2 * (own - source - 1) + (place == high_at).astype(jnp.int32)
    index = jnp.where(source == own, place, away)
    slots = jnp.arange(N_SEL, dtype=jnp.int32)
    earlier = slots[None, :] < slots[:, None]
    repeated = jnp.any((chosen[..., :, None] == chosen[..., None, :]) & earlier, axis=-1)
    first = jnp.logical_not(repeated)
    rank = jnp.sum((first[..., None, :] & earlier).astype(jnp.int32), axis=-1)
    at = (rank[..., None, :] == slots[:, None]) & first[..., None, :]
    fill = own_blocks + 2 * (count - 1)
    table = jnp.where(jnp.any(at, axis=-1), jnp.sum(jnp.where(at, index[..., None, :], 0), axis=-1), fill)
    table = table.reshape(own_blocks, heads * N_SEL)

    half_blocks = own_blocks // 2
    half = part // 2
    core = part % 2
    third = rows // parts

    def halves(which):
        return attend(count, half_blocks, (which * half_blocks).reshape(1), own1, table, q, gates, kv, summaries,
                      received)

    def product(att, columns):
        return jnp.dot(att, columns, preferred_element_type=F32).astype(BF16)

    def rows_of(att, which):
        return lax.dynamic_slice_in_dim(att, which * third, third, 0)

    swap = [(i, i ^ 1) for i in range(parts)]
    cross = [(i, i ^ 2) for i in range(parts)]
    width = out_weight.shape[1]
    moved = width // 2
    left, right = out_weight[:, :moved], out_weight[:, moved:]
    other_left = lax.ppermute(left, "tp", cross)
    far = halves(1 - half)
    other_near = lax.ppermute(far, "tp", cross)
    piece = product(rows_of(far, 1 - core), right)
    got = lax.ppermute(piece, "tp", swap)
    both = (got.astype(F32) + product(rows_of(far, core), right).astype(F32)).astype(BF16)
    crossed = lax.ppermute(both, "tp", cross)
    near = halves(half)

    def near_product(which):
        mine, its = rows_of(near, which), rows_of(other_near, which)
        total = jnp.dot(mine, left, preferred_element_type=F32) + jnp.dot(its, other_left, preferred_element_type=F32)
        return total.astype(BF16), product(mine, right)

    send_left, send_right = near_product(1 - core)
    got_left = lax.ppermute(send_left, "tp", swap)
    got_right = lax.ppermute(send_right, "tp", swap)
    keep_left, keep_right = near_product(core)
    out_left = (got_left.astype(F32) + keep_left.astype(F32)).astype(BF16)
    out_right = (got_right.astype(F32) + keep_right.astype(F32) + crossed.astype(F32)).astype(BF16)
    return jnp.concatenate([out_left, out_right], axis=1)


def solution(mesh):
    placed = (
        P("kv", None),
        P(None, "tp"),
        P(None, "tp"),
        P(None, "tp"),
        P(),
        P(),
        P(),
        P(),
        P("tp", None),
        P("kv", "tp", None),
    )
    count = mesh.shape["kv"]

    def body(*args):
        return local(count, mesh.shape["tp"], *args)

    return jax.shard_map(
        body, mesh=mesh, in_specs=placed, out_specs=P(("kv", "tp"), None), check_vma=False
    )
```

```python
import functools

import jax
import jax.numpy as jnp
from jax import lax
from jax.experimental import pallas as pl
from jax.experimental.pallas import tpu as pltpu
from jax.sharding import PartitionSpec as P


HD = 64
CMP = 32
SB = 64
N_SEL = 16
LANES = 2 * HD
SPAN_PAD = 32
UNITS = 16
FIRST_UNITS, MORE_UNITS = 3, 6
LOW = -1e30
FLOOR = -1e29
EXP_SCALE = HD ** (-0.5) * 1.4426950408889634
VMEM_LIMIT = 60 * 1024 * 1024
ATTEND_LIMIT = 24 * 1024 * 1024
PROD_LIMIT = 16 * 1024 * 1024


F32 = jnp.float32
BF16 = jnp.bfloat16


def lane_iota(rows):
    return lax.broadcasted_iota(jnp.int32, (rows, LANES), 1)


def row_iota(rows):
    return lax.broadcasted_iota(jnp.int32, (rows, LANES), 0)


def proj_kernel(part_ref, tok_ref, wq_ref, wk_ref, wv_ref, gw_ref, pos_ref, km_ref, vm_ref, wo_ref, q_ref,
                gate_ref, kv_ref, sm_ref, more_ref, tok, weight, gate_rows, acc_ref, gacc_ref, held, sems, wide_sems):
    heads, rows = q_ref.shape[0], q_ref.shape[1]
    key_heads = kv_ref.shape[0]
    gates = gate_ref.shape[1]
    steps, chunk = weight.shape[0], weight.shape[1]
    at_k, at_v = heads * HD, heads * HD + key_heads * HD
    copies = []
    for i in range(steps):
        depth = slice(i * chunk, (i + 1) * chunk)
        copies.append(
            [
                pltpu.make_async_copy(tok_ref.at[:, depth], tok.at[i], sems.at[i, 0]),
                pltpu.make_async_copy(wq_ref.at[depth, :], weight.at[i, :, :at_k], sems.at[i, 1]),
                pltpu.make_async_copy(wk_ref.at[depth, :], weight.at[i, :, at_k:at_v], sems.at[i, 2]),
                pltpu.make_async_copy(wv_ref.at[depth, :], weight.at[i, :, at_v:], sems.at[i, 3]),
            ]
        )
    start = pl.multiple_of(part_ref[0] * gates, gates)
    gate_copy = pltpu.make_async_copy(gw_ref.at[pl.ds(start, gates), :], gate_rows, wide_sems.at[0])
    ahead = 2
    for i in range(ahead):
        for copy in copies[i]:
            copy.start()
        if i == 0:
            gate_copy.start()
    unit = wo_ref.shape[1] // UNITS
    more = slice(FIRST_UNITS * unit, (FIRST_UNITS + MORE_UNITS) * unit)
    fetch = pltpu.make_async_copy(wo_ref.at[:, more], held, wide_sems.at[1])
    put = pltpu.make_async_copy(held, more_ref, wide_sems.at[2])
    for i, group in enumerate(copies):
        for copy in group:
            copy.wait()
        if i == 0:
            gate_copy.wait()
        if i + ahead < steps:
            for copy in copies[i + ahead]:
                copy.start()
        elif i + ahead == steps:
            fetch.start()
        piece = jnp.dot(tok[i], weight[i], preferred_element_type=F32)
        gpiece = lax.dot_general(
            tok[i], gate_rows[:, i * chunk : (i + 1) * chunk], (((1,), (1,)), ((), ())), preferred_element_type=F32
        )
        if i == 0:
            acc_ref[...] = piece
            gacc_ref[...] = gpiece
        else:
            acc_ref[...] += piece
            gacc_ref[...] += gpiece
    fetch.wait()
    put.start()

    lane, inner = lane_iota(rows), lax.rem(row_iota(rows), SB)
    low_half = lane < HD
    ext = jnp.where((lane == HD) | (lane - HD > inner), 1.0, 0.0)
    for h in range(heads):
        slab = acc_ref[:, (h // 2) * LANES : (h // 2 + 1) * LANES]
        if h % 2:
            slab = pltpu.roll(slab, HD, 1)
        q_ref[h] = jnp.where(low_half, slab, ext).astype(BF16)
    gate_ref[...] = jax.nn.sigmoid(gacc_ref[...])

    spans = rows // CMP
    pos = pos_ref[...].astype(F32)
    pos = jnp.concatenate([pos, pos], axis=1)
    line = lax.broadcasted_iota(jnp.int32, km_ref.shape, 0)
    eye = lax.broadcasted_iota(jnp.int32, (CMP, CMP), 0) == lax.broadcasted_iota(jnp.int32, (CMP, CMP), 1)

    def column(ref, head):
        kept = jnp.sum(jnp.where(line == head, ref[...].astype(F32), 0.0), axis=0, keepdims=True)
        return jnp.sum(jnp.where(eye, kept, 0.0), axis=1, keepdims=True)

    for g in range(key_heads):
        k = acc_ref[:, at_k + (g // 2) * LANES : at_k + (g // 2 + 1) * LANES]
        v = acc_ref[:, at_v + (g // 2) * LANES : at_v + (g // 2 + 1) * LANES]
        if g % 2 == 0:
            both = jnp.where(low_half, k, pltpu.roll(v, HD, 1))
        else:
            both = jnp.where(low_half, pltpu.roll(k, HD, 1), v)
        both = both.astype(BF16)
        kv_ref[g] = both
        head = part_ref[0] * key_heads + g
        mix = jnp.where(lane_iota(CMP) < HD, column(km_ref, head), column(vm_ref, head))
        windows = both.astype(F32).reshape(spans, CMP, LANES) + pos[None]
        total = jnp.sum(windows * mix[None], axis=1)
        pad = jnp.zeros((SPAN_PAD - spans, LANES), F32)
        sm_ref[g] = jnp.concatenate([total, pad], axis=0).astype(BF16)
    put.wait()


def project(part, tokens, query_weight, key_weight, value_weight, gate_rows, pos, kmix, vmix, out_weight):
    rows, depth = tokens.shape
    qwidth, width = query_weight.shape[1], key_weight.shape[1]
    heads, key_heads = qwidth // HD, width // HD
    steps = 4
    chunk = depth // steps
    inner, wide = out_weight.shape
    hbm = pl.BlockSpec(memory_space=pl.ANY)
    smem = pl.BlockSpec(memory_space=pltpu.SMEM)
    full = lambda shape: pl.BlockSpec(shape, lambda i: (0,) * len(shape))
    return pl.pallas_call(
        proj_kernel,
        grid=(1,),
        in_specs=[smem, hbm, hbm, hbm, hbm, hbm, full(pos.shape), full(kmix.shape), full(vmix.shape), hbm],
        out_specs=[
            full((heads, rows, LANES)),
            full((rows, 2 * heads)),
            full((key_heads, rows, LANES)),
            full((key_heads, SPAN_PAD, LANES)),
            hbm,
        ],
        scratch_shapes=[
            pltpu.VMEM((steps, rows, chunk), BF16),
            pltpu.VMEM((steps, chunk, qwidth + 2 * width), BF16),
            pltpu.VMEM((2 * heads, depth), BF16),
            pltpu.VMEM((rows, qwidth + 2 * width), F32),
            pltpu.VMEM((rows, 2 * heads), F32),
            pltpu.VMEM((inner, MORE_UNITS * wide // UNITS), BF16),
            pltpu.SemaphoreType.DMA((steps, 4)),
            pltpu.SemaphoreType.DMA((3,)),
        ],
        out_shape=[
            jax.ShapeDtypeStruct((heads, rows, LANES), BF16),
            jax.ShapeDtypeStruct((rows, 2 * heads), F32),
            jax.ShapeDtypeStruct((key_heads, rows, LANES), BF16),
            jax.ShapeDtypeStruct((key_heads, SPAN_PAD, LANES), BF16),
            jax.ShapeDtypeStruct((inner, MORE_UNITS * wide // UNITS), BF16),
        ],
        cost_estimate=pl.CostEstimate(
            flops=2 * rows * depth * (qwidth + 3 * width), transcendentals=0, bytes_accessed=2 * depth * (rows + qwidth)
        ),
        compiler_params=pltpu.CompilerParams(vmem_limit_bytes=VMEM_LIMIT),
        name="project",
    )(part, tokens, query_weight, key_weight, value_weight, gate_rows, pos, kmix, vmix, out_weight)


def copy_kernel(from_ref, to_ref):
    to_ref[...] = from_ref[...]


def first_piece(out_weight):
    inner, wide = out_weight.shape
    width = FIRST_UNITS * wide // UNITS
    spec = pl.BlockSpec((inner // 2, width), lambda i: (i, 0))
    return pl.pallas_call(
        copy_kernel,
        grid=(2,),
        in_specs=[spec],
        out_specs=spec,
        out_shape=jax.ShapeDtypeStruct((inner, width), BF16),
        compiler_params=pltpu.CompilerParams(vmem_limit_bytes=VMEM_LIMIT),
        name="first_piece",
    )(out_weight)


def select_kernel(count, own_ref, req_ref, kv_ref, sm_ref, *out_refs):
    heads = kv_ref.shape[0]
    own = own_ref[0]
    for shift in range(1, count):
        taker = jnp.minimum(own + shift, count - 1)
        out_ref = out_refs[shift - 1]
        for g in range(heads):
            for j in range(2):
                block = req_ref[taker, own * (2 * heads) + 2 * g + j]
                out_ref[g, j * SB : (j + 1) * SB, :] = kv_ref[g, pl.ds(pl.multiple_of(block * SB, SB), SB), :]
            out_ref[g, 2 * SB :, :] = sm_ref[g]


def select_blocks(count, own, requests, kv, summaries):
    heads = kv.shape[0]
    piece = (heads, 2 * SB + SPAN_PAD, LANES)
    smem = pl.BlockSpec(memory_space=pltpu.SMEM)
    full = lambda shape: pl.BlockSpec(shape, lambda i: (0,) * len(shape))
    return pl.pallas_call(
        functools.partial(select_kernel, count),
        grid=(1,),
        in_specs=[smem, smem, full(kv.shape), full(summaries.shape)],
        out_specs=[full(piece)] * (count - 1),
        out_shape=[jax.ShapeDtypeStruct(piece, BF16)] * (count - 1),
        compiler_params=pltpu.CompilerParams(vmem_limit_bytes=VMEM_LIMIT),
        name="select_blocks",
    )(own, requests, kv, summaries)


def attn_kernel(count, blocks, *refs):
    half_ref, own_ref, core_ref, table_ref, q_ref, gate_ref, kv_ref, sm_ref = refs[:8]
    recv_refs = refs[8 : 8 + count - 1]
    out_ref, poolk, poolv, sumk, sumv, score0, score1, weight0, weight1 = refs[8 + count - 1 :]
    own, base = own_ref[0], half_ref[0] * blocks
    turn = (1 - core_ref[0]) * (blocks * SB // 2)
    heads, rows = kv_ref.shape[0], kv_ref.shape[1]
    group = q_ref.shape[0] // heads
    own_blocks = rows // SB
    spans = rows // CMP
    total_blocks = poolk.shape[1] - 1
    named = N_SEL * SB
    lane, row = lane_iota(SB), row_iota(SB)
    keep = jnp.where(lane < HD, 1.0, 0.0).astype(BF16)
    other = jnp.where(lane < HD, 0.0, 1.0).astype(BF16)
    span_lane, span_row = lane_iota(SPAN_PAD), row_iota(SPAN_PAD)
    low_half = lane < HD
    diagonal = jnp.where((lane - HD == row) & (row > 0), LOW, 0.0).astype(BF16)
    contract = (((1,), (1,)), ((), ()))

    def wide(piece):
        n = piece.shape[0]
        turned = pltpu.roll(piece.astype(F32), HD, 1).astype(BF16)
        return jnp.concatenate([piece * other[:n] + keep[:n], turned * keep[:n] + other[:n]], axis=1)

    for g in range(heads):
        for j in range(own_blocks):
            piece = kv_ref[g, j * SB : (j + 1) * SB, :]
            poolk[g, j] = piece * keep
            poolv[g, j] = wide(piece)
        for k, recv in enumerate(recv_refs):
            for j in range(2):
                piece = recv[g, j * SB : (j + 1) * SB, :]
                poolk[g, own_blocks + 2 * k + j] = piece * keep
                poolv[g, own_blocks + 2 * k + j] = wide(piece)
        poolk[g, total_blocks] = jnp.where(lane == HD, LOW, 0.0).astype(BF16)
        poolv[g, total_blocks] = jnp.zeros((SB, 2 * LANES), BF16)
        for k in range(count):
            piece = sm_ref[g] if k == 0 else recv_refs[k - 1][g, 2 * SB :, :]
            sumv[g, k * SPAN_PAD : (k + 1) * SPAN_PAD] = wide(piece)
            if k:
                hidden = (span_lane == HD) & ((span_row >= spans) | (own < k))
                bias = jnp.where(hidden, LOW, 0.0).astype(BF16)
                sumk[g, (k - 1) * SPAN_PAD : k * SPAN_PAD] = piece * keep[:SPAN_PAD] + bias

    def scores(j, g, score):
        block = base + j
        last = SB // CMP * block
        hidden = (span_lane == HD) & (span_row >= last + SB // CMP)
        for i in range(SB // CMP):
            hidden = hidden | ((span_row == last + i) & (span_lane == HD + (i + 1) * CMP - 1))
        bias = jnp.where(hidden, LOW, 0.0).astype(BF16)
        pieces = [poolk[g, table_ref[block, g * N_SEL + s]] for s in range(N_SEL)]
        pieces[0] = pieces[0] + diagonal
        keys = jnp.concatenate([*pieces, sm_ref[g] * keep[:SPAN_PAD] + bias, sumk[g]], axis=0)
        q = q_ref[g * group : (g + 1) * group, pl.ds(pl.multiple_of(j * SB, SB), SB), :]
        q = q.reshape(group * SB, LANES)
        score[...] = lax.dot_general(q, keys, contract, preferred_element_type=F32)

    def weights(score, weight):
        top = jnp.max(score[:, :named], axis=1, keepdims=True)
        weight[:, :named] = jnp.exp2((score[:, :named] - top) * EXP_SCALE).astype(BF16)
        top = jnp.maximum(jnp.max(score[:, named:], axis=1, keepdims=True), FLOOR)
        weight[:, named:] = jnp.exp2((score[:, named:] - top) * EXP_SCALE).astype(BF16)

    def mixed(j, g, weight):
        block = base + j
        values = jnp.concatenate([poolv[g, table_ref[block, g * N_SEL + s]] for s in range(N_SEL)], axis=0)
        picked = jnp.dot(weight[:, :named], values, preferred_element_type=F32)
        summed = jnp.dot(weight[:, named:], sumv[g], preferred_element_type=F32)
        gate = gate_ref[pl.ds(pl.multiple_of(j * SB, SB), SB), :]
        for pair in range(group // 2):
            h = g * group + 2 * pair
            even, odd = slice(2 * pair * SB, (2 * pair + 1) * SB), slice((2 * pair + 1) * SB, (2 * pair + 2) * SB)

            def branch(out, which):
                top = jnp.where(low_half, out[even, LANES:], out[odd, :LANES])
                total = jnp.where(low_half, out[even, :LANES], out[odd, LANES:])
                scale = jnp.where(low_half, gate[:, 2 * h + which : 2 * h + which + 1],
                                  gate[:, 2 * h + 2 + which : 2 * h + 3 + which])
                return top * (scale / jnp.maximum(total, 1e-30))

            both = (branch(summed, 0) + branch(picked, 1)).astype(BF16)
            at = (g * group) // 2 + pair
            for part in range(SB // CMP):
                place = lax.rem(j * SB + part * CMP + turn, blocks * SB)
                place = pl.ds(pl.multiple_of(place, CMP), CMP)
                out_ref[place, at * LANES : (at + 1) * LANES] = both[part * CMP : (part + 1) * CMP]

    slots = [(score0, weight0), (score1, weight1)]

    def stage(first, ahead, behind):
        if first is not None:
            scores(*first, slots[first[1] % 2][0])
        if ahead is not None:
            weights(*slots[ahead[1] % 2])
        if behind is not None:
            mixed(*behind, slots[behind[1] % 2][1])

    def unit(j, g):
        return (j + g // heads, g % heads) if g >= 0 else (j - 1, g + heads)

    stage(unit(0, 0), None, None)
    stage(unit(0, 1), unit(0, 0), None)

    def body(j, carry):
        for g in range(heads):
            stage(unit(j, g), unit(j, g - 1), unit(j, g - 2))
        return carry

    lax.fori_loop(1, blocks, body, 0)
    stage(None, unit(blocks - 1, 1), unit(blocks - 1, 0))
    stage(None, None, unit(blocks - 1, 1))


def attend(count, blocks, half, own, core, table, q, gates, kv, summaries, received):
    heads, rows = kv.shape[0], kv.shape[1]
    group = q.shape[0] // heads
    total = rows // SB + 2 * (count - 1)
    keys = N_SEL * SB + count * SPAN_PAD
    full = lambda shape: pl.BlockSpec(shape, lambda i, *s: (0,) * len(shape))
    return pl.pallas_call(
        functools.partial(attn_kernel, count, blocks),
        grid_spec=pltpu.PrefetchScalarGridSpec(
            num_scalar_prefetch=4,
            grid=(1,),
            in_specs=[
                pl.BlockSpec((q.shape[0], blocks * SB, LANES), lambda i, half, *s: (0, half[0], 0)),
                pl.BlockSpec((blocks * SB, gates.shape[1]), lambda i, half, *s: (half[0], 0)),
                full(kv.shape),
                full(summaries.shape),
                *[full(r.shape) for r in received],
            ],
            out_specs=full((blocks * SB, q.shape[0] * HD)),
        scratch_shapes=[
            pltpu.VMEM((heads, total + 1, SB, LANES), BF16),
            pltpu.VMEM((heads, total + 1, SB, 2 * LANES), BF16),
            pltpu.VMEM((heads, (count - 1) * SPAN_PAD, LANES), BF16),
            pltpu.VMEM((heads, count * SPAN_PAD, 2 * LANES), BF16),
            pltpu.VMEM((group * SB, keys), F32),
            pltpu.VMEM((group * SB, keys), F32),
            pltpu.VMEM((group * SB, keys), BF16),
            pltpu.VMEM((group * SB, keys), BF16),
        ]),
        out_shape=jax.ShapeDtypeStruct((blocks * SB, q.shape[0] * HD), BF16),
        cost_estimate=pl.CostEstimate(
            flops=blocks * q.shape[0] * SB * keys * LANES * 4,
            transcendentals=blocks * q.shape[0] * SB * keys,
            bytes_accessed=4 * kv.size,
        ),
        compiler_params=pltpu.CompilerParams(vmem_limit_bytes=ATTEND_LIMIT),
        name="attend",
    )(half, own, core, table, q, gates, kv, summaries, *received)


def product_kernel(starts, near_ref, own_ref, *refs):
    send_ref, keep_ref = refs[-2:]
    rows = send_ref.shape[0]
    step = pl.program_id(0)
    total = jnp.dot(near_ref[...], own_ref[...], preferred_element_type=F32)
    if not starts:
        send_ref[...] = total[:rows].astype(BF16)
        keep_ref[...] = total[rows:].astype(BF16)
        return
    its_ref, piece_refs = refs[0], refs[1:-2]

    def one(piece_ref):
        both = total + jnp.dot(its_ref[...], piece_ref[...], preferred_element_type=F32)
        send_ref[...] = both[:rows].astype(BF16)
        keep_ref[...] = both[rows:].astype(BF16)

    for k, piece_ref in enumerate(piece_refs):
        inside = step >= starts[k]
        if k + 1 < len(piece_refs):
            inside = inside & (step < starts[k + 1])
        pl.when(inside)(functools.partial(one, piece_ref))


def out_product(near, out_weight, first, units, its=None, pieces=()):
    depth, wide = out_weight.shape
    unit = wide // UNITS * 3 if units % 3 == 0 else wide // UNITS * units
    steps = units * (wide // UNITS) // unit
    offset = first * (wide // UNITS)
    sizes = [piece.shape[1] // unit for piece in pieces]
    starts = [sum(sizes[:k]) for k in range(len(sizes))]
    rows = near.shape[0] // 2
    full = lambda shape: pl.BlockSpec(shape, lambda i: (0,) * len(shape))

    def piece_spec(k):
        return pl.BlockSpec((depth, unit), lambda i: (0, jnp.clip(i - starts[k], 0, sizes[k] - 1)))

    out = pl.BlockSpec((rows, unit), lambda i: (0, i))
    args = [near, out_weight] + ([its, *pieces] if pieces else [])
    specs = [full(near.shape), pl.BlockSpec((pl.Element(depth), pl.Element(unit)), lambda i: (0, pl.multiple_of(offset + i * unit, 2 * LANES)))]
    if pieces:
        specs += [full(its.shape), *[piece_spec(k) for k in range(len(pieces))]]
    return pl.pallas_call(
        functools.partial(product_kernel, starts),
        grid=(steps,),
        in_specs=specs,
        out_specs=[out, out],
        out_shape=[jax.ShapeDtypeStruct((rows, steps * unit), BF16)] * 2,
        cost_estimate=pl.CostEstimate(
            flops=8 * rows * depth * steps * unit, transcendentals=0, bytes_accessed=4 * depth * steps * unit
        ),
        compiler_params=pltpu.CompilerParams(vmem_limit_bytes=PROD_LIMIT),
        name="out_product",
    )(*args)


def final_kernel(first, *refs):
    out_ref, total, sem = refs[-3:]
    width = total.shape[1]
    value = refs[0][...].astype(F32) + refs[1][...].astype(F32)
    if len(refs) > 6:
        value += refs[2][...].astype(F32)
    total[...] = value.astype(BF16)
    copy = pltpu.make_async_copy(total, out_ref.at[:, first : first + width], sem)
    copy.start()
    copy.wait()


def final_sum(wide, first, *parts, into=None):
    rows, width = parts[0].shape
    full = pl.BlockSpec((rows, width), lambda i: (0, 0))
    hbm = pl.BlockSpec(memory_space=pl.ANY)
    more = [] if into is None else [into]
    return pl.pallas_call(
        functools.partial(final_kernel, first),
        grid=(1,),
        in_specs=[full] * len(parts) + [hbm] * len(more),
        out_specs=hbm,
        out_shape=jax.ShapeDtypeStruct((rows, wide), BF16),
        scratch_shapes=[pltpu.VMEM((rows, width), BF16), pltpu.SemaphoreType.DMA],
        input_output_aliases={} if into is None else {len(parts): 0},
        compiler_params=pltpu.CompilerParams(vmem_limit_bytes=PROD_LIMIT),
        name="final_sum",
    )(*parts, *more)


def local(count, parts, tokens, query_weight, key_weight, value_weight, gate_weight, summary_pos, key_mixing,
          value_mixing, out_weight, chosen):
    rows = tokens.shape[0]
    own = lax.axis_index("kv").astype(jnp.int32)
    part = lax.axis_index("tp").astype(jnp.int32)
    own_blocks = rows // SB
    heads = key_weight.shape[1] // HD
    own1, part1 = own.reshape(1), part.reshape(1)

    source = chosen // own_blocks
    place = chosen - source * own_blocks
    match = source[None] == jnp.arange(count, dtype=jnp.int32)[:, None, None, None]
    lowest = jnp.min(jnp.where(match, place[None], own_blocks - 1), axis=(1, 3))
    highest = jnp.max(jnp.where(match, place[None], 0), axis=(1, 3))
    request = jnp.stack([lowest, highest], axis=-1).reshape(1, count * heads * 2)
    everyone = jnp.where(jnp.arange(count, dtype=jnp.int32)[:, None] == own, request, 0)
    if count & (count - 1) == 0:
        bit, stage = 1, 0
        while bit < count:
            got = lax.ppermute(everyone, "kv", [(i, i ^ bit) for i in range(count)])
            everyone = everyone + got
            if stage == 0:
                chosen = lax.optimization_barrier((chosen, got))[0]
            bit, stage = 2 * bit, stage + 1
    else:
        everyone = lax.all_gather(request, "kv", axis=0, tiled=True)

    cross = [(i, i ^ 2) for i in range(parts)]
    swap = [(i, i ^ 1) for i in range(parts)]
    piece_a = lax.ppermute(first_piece(out_weight), "tp", cross)
    q, gates, kv, summaries, more = project(
        part1, tokens, query_weight, key_weight, value_weight, gate_weight.T, summary_pos, key_mixing.T,
        value_mixing.T, out_weight,
    )
    piece_b = lax.ppermute(more, "tp", cross)

    pieces = select_blocks(count, own1, everyone, kv, summaries)
    received = []
    for k in range(1, count):
        received.append(lax.ppermute(pieces[k - 1], "kv", [(i, i + k) for i in range(count - k)]))

    source = chosen // own_blocks
    place = chosen - source * own_blocks
    match = source[None] == jnp.arange(count, dtype=jnp.int32)[:, None, None, None]

    high_at = jnp.sum(jnp.where(match, highest[:, None, :, None], 0), axis=0)
    away = own_blocks + 2 * (own - source - 1) + (place == high_at).astype(jnp.int32)
    index = jnp.where(source == own, place, away)
    slots = jnp.arange(N_SEL, dtype=jnp.int32)
    earlier = slots[None, :] < slots[:, None]
    repeated = jnp.any((chosen[..., :, None] == chosen[..., None, :]) & earlier, axis=-1)
    first = jnp.logical_not(repeated)
    rank = jnp.sum((first[..., None, :] & earlier).astype(jnp.int32), axis=-1)
    at = (rank[..., None, :] == slots[:, None]) & first[..., None, :]
    fill = own_blocks + 2 * (count - 1)
    table = jnp.where(jnp.any(at, axis=-1), jnp.sum(jnp.where(at, index[..., None, :], 0), axis=-1), fill)
    table = table.reshape(own_blocks, heads * N_SEL)

    half_blocks = own_blocks // 2
    half = part // 2
    core1 = (part % 2).reshape(1)

    def halves(which):
        return attend(count, half_blocks, which.reshape(1), own1, core1, table, q, gates, kv, summaries,
                      received)

    left = FIRST_UNITS + MORE_UNITS
    right = UNITS - left
    wide = out_weight.shape[1]
    far = halves(1 - half)
    its = lax.ppermute(far, "tp", cross)
    send, keep = out_product(far, out_weight, left, right)
    got = lax.ppermute(send, "tp", swap)
    crossed = lax.ppermute((got.astype(F32) + keep.astype(F32)).astype(BF16), "tp", cross)
    near = halves(half)
    send, keep = out_product(near, out_weight, 0, left, its, [piece_a, piece_b])
    got = lax.ppermute(send, "tp", swap)
    late_send, late_keep = out_product(near, out_weight, left, right)
    late_got = lax.ppermute(late_send, "tp", swap)
    out = final_sum(wide, 0, got, keep)
    return final_sum(wide, left * wide // UNITS, late_got, late_keep, crossed, into=out)


def solution(mesh):
    placed = (
        P("kv", None),
        P(None, "tp"),
        P(None, "tp"),
        P(None, "tp"),
        P(),
        P(),
        P(),
        P(),
        P("tp", None),
        P("kv", "tp", None),
    )
    count = mesh.shape["kv"]

    def body(*args):
        return local(count, mesh.shape["tp"], *args)

    return jax.shard_map(
        body, mesh=mesh, in_specs=placed, out_specs=P(("kv", "tp"), None), check_vma=False
    )
```

```python
import functools

import jax
import jax.numpy as jnp
from jax import lax
from jax.experimental import pallas as pl
from jax.experimental.pallas import tpu as pltpu
from jax.sharding import PartitionSpec as P


HD = 64
CMP = 32
SB = 64
N_SEL = 16
LANES = 2 * HD
SPAN_PAD = 32
UNITS = 16
BLOCK = 512
FIRST_UNITS, MORE_UNITS = 2, 7
LOW = -1e30
FLOOR = -1e29
EXP_SCALE = HD ** (-0.5) * 1.4426950408889634
VMEM_LIMIT = 60 * 1024 * 1024
SELECT_LIMIT = 8 * 1024 * 1024
ATTEND_LIMIT = 24 * 1024 * 1024
PROJ_LIMIT = 57 * 1024 * 1024
PROD_LIMIT = 16 * 1024 * 1024


F32 = jnp.float32
BF16 = jnp.bfloat16


def lane_iota(rows):
    return lax.broadcasted_iota(jnp.int32, (rows, LANES), 1)


def row_iota(rows):
    return lax.broadcasted_iota(jnp.int32, (rows, LANES), 0)


def staged(copies, ahead, step):
    for group in copies[:ahead]:
        for copy in group:
            copy.start()
    for i, group in enumerate(copies):
        for copy in group:
            copy.wait()
        if i + ahead < len(copies):
            for copy in copies[i + ahead]:
                copy.start()
        step(i)


def kv_kernel(part_ref, tok_ref, wk_ref, wv_ref, pos_ref, km_ref, vm_ref, wo_ref, kv_ref, sm_ref, more_ref, tok, weight,
              acc_ref, held, sems, wide_sems):
    key_heads, rows = kv_ref.shape[0], kv_ref.shape[1]
    steps, chunk = weight.shape[0], weight.shape[1]
    at_v = key_heads * HD
    copies = []
    for i in range(steps):
        depth = slice(i * chunk, (i + 1) * chunk)
        copies.append(
            [
                pltpu.make_async_copy(tok_ref.at[:, depth], tok.at[i], sems.at[i, 0]),
                pltpu.make_async_copy(wk_ref.at[depth, :], weight.at[i, :, :at_v], sems.at[i, 1]),
                pltpu.make_async_copy(wv_ref.at[depth, :], weight.at[i, :, at_v:], sems.at[i, 2]),
            ]
        )

    unit = wo_ref.shape[1] // UNITS
    more = slice(FIRST_UNITS * unit, (FIRST_UNITS + MORE_UNITS) * unit)
    fetch = pltpu.make_async_copy(wo_ref.at[:, more], held, wide_sems.at[0])
    put = pltpu.make_async_copy(held, more_ref, wide_sems.at[1])

    def step(i):
        if i == steps - 2:
            fetch.start()
        piece = jnp.dot(tok[i], weight[i], preferred_element_type=F32)
        acc_ref[...] = piece if i == 0 else acc_ref[...] + piece

    staged(copies, 2, step)
    fetch.wait()
    put.start()
    low_half = lane_iota(rows) < HD
    spans = rows // CMP
    pos = pos_ref[...].astype(F32)
    pos = jnp.concatenate([pos, pos], axis=1)
    line = lax.broadcasted_iota(jnp.int32, km_ref.shape, 0)
    eye = lax.broadcasted_iota(jnp.int32, (CMP, CMP), 0) == lax.broadcasted_iota(jnp.int32, (CMP, CMP), 1)

    def column(ref, head):
        kept = jnp.sum(jnp.where(line == head, ref[...].astype(F32), 0.0), axis=0, keepdims=True)
        return jnp.sum(jnp.where(eye, kept, 0.0), axis=1, keepdims=True)

    for g in range(key_heads):
        k = acc_ref[:, (g // 2) * LANES : (g // 2 + 1) * LANES]
        v = acc_ref[:, at_v + (g // 2) * LANES : at_v + (g // 2 + 1) * LANES]
        if g % 2 == 0:
            both = jnp.where(low_half, k, pltpu.roll(v, HD, 1))
        else:
            both = jnp.where(low_half, pltpu.roll(k, HD, 1), v)
        both = both.astype(BF16)
        kv_ref[g] = both
        head = part_ref[0] * key_heads + g
        mix = jnp.where(lane_iota(CMP) < HD, column(km_ref, head), column(vm_ref, head))
        windows = both.astype(F32).reshape(spans, CMP, LANES) + pos[None]
        total = jnp.sum(windows * mix[None], axis=1)
        pad = jnp.zeros((SPAN_PAD - spans, LANES), F32)
        sm_ref[g] = jnp.concatenate([total, pad], axis=0).astype(BF16)
    put.wait()


def project_kv(part, tokens, key_weight, value_weight, pos, kmix, vmix, out_weight):
    rows, depth = tokens.shape
    inner, wide = out_weight.shape
    width = key_weight.shape[1]
    key_heads = width // HD
    steps = 4
    chunk = depth // steps
    hbm = pl.BlockSpec(memory_space=pl.ANY)
    smem = pl.BlockSpec(memory_space=pltpu.SMEM)
    full = lambda shape: pl.BlockSpec(shape, lambda i: (0,) * len(shape))
    return pl.pallas_call(
        kv_kernel,
        grid=(1,),
        in_specs=[smem, hbm, hbm, hbm, full(pos.shape), full(kmix.shape), full(vmix.shape), hbm],
        out_specs=[full((key_heads, rows, LANES)), full((key_heads, SPAN_PAD, LANES)), hbm],
        scratch_shapes=[
            pltpu.VMEM((steps, rows, chunk), BF16),
            pltpu.VMEM((steps, chunk, 2 * width), BF16),
            pltpu.VMEM((rows, 2 * width), F32),
            pltpu.VMEM((inner, MORE_UNITS * wide // UNITS), BF16),
            pltpu.SemaphoreType.DMA((steps, 3)),
            pltpu.SemaphoreType.DMA((2,)),
        ],
        out_shape=[
            jax.ShapeDtypeStruct((key_heads, rows, LANES), BF16),
            jax.ShapeDtypeStruct((key_heads, SPAN_PAD, LANES), BF16),
            jax.ShapeDtypeStruct((inner, MORE_UNITS * wide // UNITS), BF16),
        ],
        cost_estimate=pl.CostEstimate(
            flops=4 * rows * depth * width, transcendentals=0, bytes_accessed=2 * depth * (rows + 2 * width)
        ),
        compiler_params=pltpu.CompilerParams(vmem_limit_bytes=VMEM_LIMIT),
        name="project_kv",
    )(part, tokens, key_weight, value_weight, pos, kmix, vmix, out_weight)


def q_kernel(part_ref, tok_ref, wq_ref, gw_ref, q_ref, gate_ref, tok, weight, gate_rows, acc_ref, gacc_ref, sems):
    heads, rows = q_ref.shape[0], q_ref.shape[1]
    gates = gate_ref.shape[1]
    steps, chunk = weight.shape[0], weight.shape[1]
    start = pl.multiple_of(part_ref[0] * gates, gates)
    copies = []
    for i in range(steps):
        depth = slice(i * chunk, (i + 1) * chunk)
        copies.append(
            [
                pltpu.make_async_copy(tok_ref.at[:, depth], tok.at[i], sems.at[i, 0]),
                pltpu.make_async_copy(wq_ref.at[depth, :], weight.at[i], sems.at[i, 1]),
                pltpu.make_async_copy(gw_ref.at[pl.ds(start, gates), depth], gate_rows.at[i], sems.at[i, 2]),
            ]
        )

    def step(i):
        piece = jnp.dot(tok[i], weight[i], preferred_element_type=F32)
        gpiece = lax.dot_general(tok[i], gate_rows[i], (((1,), (1,)), ((), ())), preferred_element_type=F32)
        acc_ref[...] = piece if i == 0 else acc_ref[...] + piece
        gacc_ref[...] = gpiece if i == 0 else gacc_ref[...] + gpiece

    staged(copies, 2, step)
    lane, inner = lane_iota(rows), lax.rem(row_iota(rows), SB)
    low_half = lane < HD
    ext = jnp.where((lane == HD) | (lane - HD > inner), 1.0, 0.0)
    for h in range(heads):
        slab = acc_ref[:, (h // 2) * LANES : (h // 2 + 1) * LANES]
        if h % 2:
            slab = pltpu.roll(slab, HD, 1)
        q_ref[h] = jnp.where(low_half, slab, ext).astype(BF16)
    gate_ref[...] = jax.nn.sigmoid(gacc_ref[...])


def project_q(part, tokens, query_weight, gate_rows):
    rows, depth = tokens.shape
    qwidth = query_weight.shape[1]
    heads = qwidth // HD
    steps = 4
    chunk = depth // steps
    hbm = pl.BlockSpec(memory_space=pl.ANY)
    smem = pl.BlockSpec(memory_space=pltpu.SMEM)
    full = lambda shape: pl.BlockSpec(shape, lambda i: (0,) * len(shape))
    return pl.pallas_call(
        q_kernel,
        grid=(1,),
        in_specs=[smem, hbm, hbm, hbm],
        out_specs=[full((heads, rows, LANES)), full((rows, 2 * heads))],
        scratch_shapes=[
            pltpu.VMEM((steps, rows, chunk), BF16),
            pltpu.VMEM((steps, chunk, qwidth), BF16),
            pltpu.VMEM((steps, 2 * heads, chunk), BF16),
            pltpu.VMEM((rows, qwidth), F32),
            pltpu.VMEM((rows, 2 * heads), F32),
            pltpu.SemaphoreType.DMA((steps, 3)),
        ],
        out_shape=[
            jax.ShapeDtypeStruct((heads, rows, LANES), BF16),
            jax.ShapeDtypeStruct((rows, 2 * heads), F32),
        ],
        cost_estimate=pl.CostEstimate(
            flops=3 * rows * depth * qwidth, transcendentals=0, bytes_accessed=2 * depth * (rows + qwidth)
        ),
        compiler_params=pltpu.CompilerParams(vmem_limit_bytes=PROJ_LIMIT),
        name="project_q",
    )(part, tokens, query_weight, gate_rows)


def copy_kernel(from_ref, to_ref):
    to_ref[...] = from_ref[...]


def first_piece(out_weight):
    inner, wide = out_weight.shape
    width = FIRST_UNITS * wide // UNITS
    spec = pl.BlockSpec((inner // 2, width), lambda i: (i, 0))
    return pl.pallas_call(
        copy_kernel,
        grid=(2,),
        in_specs=[spec],
        out_specs=spec,
        out_shape=jax.ShapeDtypeStruct((inner, width), BF16),
        compiler_params=pltpu.CompilerParams(vmem_limit_bytes=VMEM_LIMIT),
        name="first_piece",
    )(out_weight)


def select_kernel(count, own_ref, req_ref, kv_ref, sm_ref, *out_refs):
    heads = kv_ref.shape[0]
    own = own_ref[0]
    for shift in range(1, count):
        taker = jnp.minimum(own + shift, count - 1)
        out_ref = out_refs[shift - 1]
        for g in range(heads):
            for j in range(2):
                block = req_ref[taker, own * (2 * heads) + 2 * g + j]
                out_ref[g, j * SB : (j + 1) * SB, :] = kv_ref[g, pl.ds(pl.multiple_of(block * SB, SB), SB), :]
            out_ref[g, 2 * SB :, :] = sm_ref[g]


def select_blocks(count, own, requests, kv, summaries):
    heads = kv.shape[0]
    piece = (heads, 2 * SB + SPAN_PAD, LANES)
    smem = pl.BlockSpec(memory_space=pltpu.SMEM)
    full = lambda shape: pl.BlockSpec(shape, lambda i: (0,) * len(shape))
    return pl.pallas_call(
        functools.partial(select_kernel, count),
        grid=(1,),
        in_specs=[smem, smem, full(kv.shape), full(summaries.shape)],
        out_specs=[full(piece)] * (count - 1),
        out_shape=[jax.ShapeDtypeStruct(piece, BF16)] * (count - 1),
        compiler_params=pltpu.CompilerParams(vmem_limit_bytes=SELECT_LIMIT),
        name="select_blocks",
    )(own, requests, kv, summaries)


def stage_kernel(q_ref, gate_ref, q_out, gate_out, sems):
    copies = [pltpu.make_async_copy(q_ref, q_out, sems.at[0]), pltpu.make_async_copy(gate_ref, gate_out, sems.at[1])]
    for copy in copies:
        copy.start()
    for copy in copies:
        copy.wait()


def bring(q, gates):
    hbm = pl.BlockSpec(memory_space=pl.ANY)
    vmem = pl.BlockSpec(memory_space=pltpu.VMEM)
    return pl.pallas_call(
        stage_kernel,
        in_specs=[hbm, hbm],
        out_specs=[vmem, vmem],
        out_shape=[jax.ShapeDtypeStruct(q.shape, BF16), jax.ShapeDtypeStruct(gates.shape, F32)],
        scratch_shapes=[pltpu.SemaphoreType.DMA((2,))],
        compiler_params=pltpu.CompilerParams(vmem_limit_bytes=SELECT_LIMIT),
        name="stage",
    )(q, gates)


def attn_kernel(count, blocks, *refs):
    half_ref, own_ref, core_ref, table_ref, q_ref, gate_ref, kv_ref, sm_ref = refs[:8]
    recv_refs = refs[8 : 8 + count - 1]
    out_ref, poolk, poolv, sumk, sumv, score0, score1, weight0, weight1 = refs[8 + count - 1 :]
    own, base = own_ref[0], half_ref[0] * blocks
    turn = (1 - core_ref[0]) * (blocks * SB // 2)
    heads, rows = kv_ref.shape[0], kv_ref.shape[1]
    group = q_ref.shape[0] // heads
    own_blocks = rows // SB
    spans = rows // CMP
    total_blocks = poolk.shape[1] - 1
    named = N_SEL * SB
    lane, row = lane_iota(SB), row_iota(SB)
    keep = jnp.where(lane < HD, 1.0, 0.0).astype(BF16)
    other = jnp.where(lane < HD, 0.0, 1.0).astype(BF16)
    span_lane, span_row = lane_iota(SPAN_PAD), row_iota(SPAN_PAD)
    low_half = lane < HD
    diagonal = jnp.where((lane - HD == row) & (row > 0), LOW, 0.0).astype(BF16)
    contract = (((1,), (1,)), ((), ()))

    def wide(piece):
        n = piece.shape[0]
        turned = pltpu.roll(piece.astype(F32), HD, 1).astype(BF16)
        return jnp.concatenate([piece * other[:n] + keep[:n], turned * keep[:n] + other[:n]], axis=1)

    for g in range(heads):
        for j in range(own_blocks):
            piece = kv_ref[g, j * SB : (j + 1) * SB, :]
            poolk[g, j] = piece * keep
            poolv[g, j] = wide(piece)
        for k, recv in enumerate(recv_refs):
            for j in range(2):
                piece = recv[g, j * SB : (j + 1) * SB, :]
                poolk[g, own_blocks + 2 * k + j] = piece * keep
                poolv[g, own_blocks + 2 * k + j] = wide(piece)
        poolk[g, total_blocks] = jnp.where(lane == HD, LOW, 0.0).astype(BF16)
        poolv[g, total_blocks] = jnp.zeros((SB, 2 * LANES), BF16)
        for k in range(count):
            piece = sm_ref[g] if k == 0 else recv_refs[k - 1][g, 2 * SB :, :]
            sumv[g, k * SPAN_PAD : (k + 1) * SPAN_PAD] = wide(piece)
            if k:
                hidden = (span_lane == HD) & ((span_row >= spans) | (own < k))
                bias = jnp.where(hidden, LOW, 0.0).astype(BF16)
                sumk[g, (k - 1) * SPAN_PAD : k * SPAN_PAD] = piece * keep[:SPAN_PAD] + bias

    def scores(j, g, score):
        block = base + j
        last = SB // CMP * block
        hidden = (span_lane == HD) & (span_row >= last + SB // CMP)
        for i in range(SB // CMP):
            hidden = hidden | ((span_row == last + i) & (span_lane == HD + (i + 1) * CMP - 1))
        bias = jnp.where(hidden, LOW, 0.0).astype(BF16)
        pieces = [poolk[g, table_ref[block, g * N_SEL + s]] for s in range(N_SEL)]
        pieces[0] = pieces[0] + diagonal
        keys = jnp.concatenate([*pieces, sm_ref[g] * keep[:SPAN_PAD] + bias, sumk[g]], axis=0)
        q = q_ref[g * group : (g + 1) * group, pl.ds(pl.multiple_of(j * SB, SB), SB), :]
        q = q.reshape(group * SB, LANES)
        score[...] = lax.dot_general(q, keys, contract, preferred_element_type=F32)

    def weights(score, weight):
        top = jnp.max(score[:, :named], axis=1, keepdims=True)
        weight[:, :named] = jnp.exp2((score[:, :named] - top) * EXP_SCALE).astype(BF16)
        top = jnp.maximum(jnp.max(score[:, named:], axis=1, keepdims=True), FLOOR)
        weight[:, named:] = jnp.exp2((score[:, named:] - top) * EXP_SCALE).astype(BF16)

    def mixed(j, g, weight):
        block = base + j
        values = jnp.concatenate([poolv[g, table_ref[block, g * N_SEL + s]] for s in range(N_SEL)], axis=0)
        picked = jnp.dot(weight[:, :named], values, preferred_element_type=F32)
        summed = jnp.dot(weight[:, named:], sumv[g], preferred_element_type=F32)
        gate = gate_ref[pl.ds(pl.multiple_of(j * SB, SB), SB), :]
        for pair in range(group // 2):
            h = g * group + 2 * pair
            even, odd = slice(2 * pair * SB, (2 * pair + 1) * SB), slice((2 * pair + 1) * SB, (2 * pair + 2) * SB)

            def branch(out, which):
                top = jnp.where(low_half, out[even, LANES:], out[odd, :LANES])
                total = jnp.where(low_half, out[even, :LANES], out[odd, LANES:])
                scale = jnp.where(low_half, gate[:, 2 * h + which : 2 * h + which + 1],
                                  gate[:, 2 * h + 2 + which : 2 * h + 3 + which])
                return top * (scale / jnp.maximum(total, 1e-30))

            both = (branch(summed, 0) + branch(picked, 1)).astype(BF16)
            at = (g * group) // 2 + pair
            for part in range(SB // CMP):
                place = lax.rem(j * SB + part * CMP + turn, blocks * SB)
                place = pl.ds(pl.multiple_of(place, CMP), CMP)
                out_ref[place, at * LANES : (at + 1) * LANES] = both[part * CMP : (part + 1) * CMP]

    slots = [(score0, weight0), (score1, weight1)]

    def stage(first, ahead, behind):
        if first is not None:
            scores(*first, slots[first[1] % 2][0])
        if ahead is not None:
            weights(*slots[ahead[1] % 2])
        if behind is not None:
            mixed(*behind, slots[behind[1] % 2][1])

    def unit(j, g):
        return (j + g // heads, g % heads) if g >= 0 else (j - 1, g + heads)

    stage(unit(0, 0), None, None)
    stage(unit(0, 1), unit(0, 0), None)

    def body(j, carry):
        for g in range(heads):
            stage(unit(j, g), unit(j, g - 1), unit(j, g - 2))
        return carry

    lax.fori_loop(1, blocks, body, 0)
    stage(None, unit(blocks - 1, 1), unit(blocks - 1, 0))
    stage(None, None, unit(blocks - 1, 1))


def attend(count, blocks, half, own, core, table, q, gates, kv, summaries, received):
    heads, rows = kv.shape[0], kv.shape[1]
    group = q.shape[0] // heads
    total = rows // SB + 2 * (count - 1)
    keys = N_SEL * SB + count * SPAN_PAD
    full = lambda shape: pl.BlockSpec(shape, lambda i, *s: (0,) * len(shape))
    return pl.pallas_call(
        functools.partial(attn_kernel, count, blocks),
        grid_spec=pltpu.PrefetchScalarGridSpec(
            num_scalar_prefetch=4,
            grid=(1,),
            in_specs=[
                pl.BlockSpec((q.shape[0], blocks * SB, LANES), lambda i, half, *s: (0, half[0], 0)),
                pl.BlockSpec((blocks * SB, gates.shape[1]), lambda i, half, *s: (half[0], 0)),
                full(kv.shape),
                full(summaries.shape),
                *[full(r.shape) for r in received],
            ],
            out_specs=full((blocks * SB, q.shape[0] * HD)),
        scratch_shapes=[
            pltpu.VMEM((heads, total + 1, SB, LANES), BF16),
            pltpu.VMEM((heads, total + 1, SB, 2 * LANES), BF16),
            pltpu.VMEM((heads, (count - 1) * SPAN_PAD, LANES), BF16),
            pltpu.VMEM((heads, count * SPAN_PAD, 2 * LANES), BF16),
            pltpu.VMEM((group * SB, keys), F32),
            pltpu.VMEM((group * SB, keys), F32),
            pltpu.VMEM((group * SB, keys), BF16),
            pltpu.VMEM((group * SB, keys), BF16),
        ]),
        out_shape=jax.ShapeDtypeStruct((blocks * SB, q.shape[0] * HD), BF16),
        cost_estimate=pl.CostEstimate(
            flops=blocks * q.shape[0] * SB * keys * LANES * 4,
            transcendentals=blocks * q.shape[0] * SB * keys,
            bytes_accessed=4 * kv.size,
        ),
        compiler_params=pltpu.CompilerParams(vmem_limit_bytes=ATTEND_LIMIT),
        name="attend",
    )(half, own, core, table, q, gates, kv, summaries, *received)


def product_kernel(first, near_ref, own_ref, send_ref, keep_ref):
    rows, width = send_ref.shape
    for at in range(0, width, BLOCK):
        size = min(BLOCK, width - at)
        total = jnp.dot(near_ref[...], own_ref[:, first + at : first + at + size], preferred_element_type=F32)
        send_ref[:, at : at + size] = total[:rows].astype(BF16)
        keep_ref[:, at : at + size] = total[rows:].astype(BF16)


def joint_kernel(near_ref, its_ref, own_ref, a_ref, b_ref, send_ref, keep_ref, other, sems):
    rows, width = send_ref.shape
    start = a_ref.shape[1]
    first = pltpu.make_async_copy(a_ref, other.at[:, :start], sems.at[0])
    more = pltpu.make_async_copy(b_ref, other.at[:, start:], sems.at[1])
    first.start()
    more.start()
    for at in range(0, width, BLOCK):
        size = min(BLOCK, width - at)
        columns = slice(at, at + size)
        total = jnp.dot(near_ref[...], own_ref[:, columns], preferred_element_type=F32)
        if at == 0:
            first.wait()
        if at == start // BLOCK * BLOCK:
            more.wait()
        total += jnp.dot(its_ref[...], other[:, columns], preferred_element_type=F32)
        send_ref[:, columns] = total[:rows].astype(BF16)
        keep_ref[:, columns] = total[rows:].astype(BF16)


def out_product(near, out_weight, first, units, its=None, pieces=()):
    depth, wide = out_weight.shape
    unit = wide // UNITS
    rows = near.shape[0] // 2
    width = units * unit
    full = lambda shape: pl.BlockSpec(shape, lambda i: (0,) * len(shape))
    hbm = pl.BlockSpec(memory_space=pl.ANY)
    vmem = pl.BlockSpec(memory_space=pltpu.VMEM)
    common = dict(
        grid=(1,),
        out_specs=[full((rows, width))] * 2,
        out_shape=[jax.ShapeDtypeStruct((rows, width), BF16)] * 2,
        cost_estimate=pl.CostEstimate(flops=8 * rows * depth * width, transcendentals=0, bytes_accessed=4 * depth * width),
        compiler_params=pltpu.CompilerParams(vmem_limit_bytes=PROD_LIMIT),
    )
    if not pieces:
        return pl.pallas_call(
            functools.partial(product_kernel, first * unit),
            in_specs=[full(near.shape), vmem],
            name="out_product",
            **common,
        )(near, out_weight)
    return pl.pallas_call(
        joint_kernel,
        in_specs=[full(near.shape), full(its.shape), vmem, hbm, hbm],
        scratch_shapes=[pltpu.VMEM((depth, width), BF16), pltpu.SemaphoreType.DMA((2,))],
        name="joint_product",
        **common,
    )(near, its, out_weight, *pieces)


def final_kernel(first, *refs):
    out_ref, total, sem = refs[-3:]
    width = total.shape[1]
    value = refs[0][...].astype(F32) + refs[1][...].astype(F32)
    if len(refs) > 6:
        value += refs[2][...].astype(F32)
    total[...] = value.astype(BF16)
    copy = pltpu.make_async_copy(total, out_ref.at[:, first : first + width], sem)
    copy.start()
    copy.wait()


def final_sum(wide, first, *parts, into=None):
    rows, width = parts[0].shape
    full = pl.BlockSpec((rows, width), lambda i: (0, 0))
    hbm = pl.BlockSpec(memory_space=pl.ANY)
    more = [] if into is None else [into]
    return pl.pallas_call(
        functools.partial(final_kernel, first),
        grid=(1,),
        in_specs=[full] * len(parts) + [hbm] * len(more),
        out_specs=hbm,
        out_shape=jax.ShapeDtypeStruct((rows, wide), BF16),
        scratch_shapes=[pltpu.VMEM((rows, width), BF16), pltpu.SemaphoreType.DMA],
        input_output_aliases={} if into is None else {len(parts): 0},
        compiler_params=pltpu.CompilerParams(vmem_limit_bytes=PROD_LIMIT),
        name="final_sum",
    )(*parts, *more)


def local(count, parts, tokens, query_weight, key_weight, value_weight, gate_weight, summary_pos, key_mixing,
          value_mixing, out_weight, chosen):
    rows = tokens.shape[0]
    own = lax.axis_index("kv").astype(jnp.int32)
    part = lax.axis_index("tp").astype(jnp.int32)
    own_blocks = rows // SB
    heads = key_weight.shape[1] // HD
    own1, part1 = own.reshape(1), part.reshape(1)

    source = chosen // own_blocks
    place = chosen - source * own_blocks
    match = source[None] == jnp.arange(count, dtype=jnp.int32)[:, None, None, None]
    lowest = jnp.min(jnp.where(match, place[None], own_blocks - 1), axis=(1, 3))
    highest = jnp.max(jnp.where(match, place[None], 0), axis=(1, 3))
    request = jnp.stack([lowest, highest], axis=-1).reshape(1, count * heads * 2)
    everyone = jnp.where(jnp.arange(count, dtype=jnp.int32)[:, None] == own, request, 0)
    if count & (count - 1) == 0:
        bit = 1
        while bit < count:
            got = lax.ppermute(everyone, "kv", [(i, i ^ bit) for i in range(count)])
            everyone = everyone + got
            if 4 * bit == count:
                chosen = lax.optimization_barrier((chosen, got))[0]
            bit = 2 * bit
    else:
        everyone = lax.all_gather(request, "kv", axis=0, tiled=True)

    cross = [(i, i ^ 2) for i in range(parts)]
    swap = [(i, i ^ 1) for i in range(parts)]
    piece_a = lax.ppermute(first_piece(out_weight), "tp", cross)
    kv, summaries, more = project_kv(
        part1, tokens, key_weight, value_weight, summary_pos, key_mixing.T, value_mixing.T, out_weight
    )
    q, gates = project_q(part1, tokens, query_weight, gate_weight.T)
    piece_b = lax.ppermute(more, "tp", cross)

    pieces = select_blocks(count, own1, everyone, kv, summaries)
    received = []
    for k in range(1, count):
        received.append(lax.ppermute(pieces[k - 1], "kv", [(i, i + k) for i in range(count - k)]))

    source = chosen // own_blocks
    place = chosen - source * own_blocks
    match = source[None] == jnp.arange(count, dtype=jnp.int32)[:, None, None, None]

    q, gates = bring(q, gates)

    high_at = jnp.sum(jnp.where(match, highest[:, None, :, None], 0), axis=0)
    away = own_blocks + 2 * (own - source - 1) + (place == high_at).astype(jnp.int32)
    index = jnp.where(source == own, place, away)
    slots = jnp.arange(N_SEL, dtype=jnp.int32)
    earlier = slots[None, :] < slots[:, None]
    repeated = jnp.any((chosen[..., :, None] == chosen[..., None, :]) & earlier, axis=-1)
    first = jnp.logical_not(repeated)
    rank = jnp.sum((first[..., None, :] & earlier).astype(jnp.int32), axis=-1)
    at = (rank[..., None, :] == slots[:, None]) & first[..., None, :]
    fill = own_blocks + 2 * (count - 1)
    table = jnp.where(jnp.any(at, axis=-1), jnp.sum(jnp.where(at, index[..., None, :], 0), axis=-1), fill)
    table = table.reshape(own_blocks, heads * N_SEL)

    half_blocks = own_blocks // 2
    half = part // 2
    core1 = (part % 2).reshape(1)

    def halves(which):
        return attend(count, half_blocks, which.reshape(1), own1, core1, table, q, gates, kv, summaries,
                      received)

    left = FIRST_UNITS + MORE_UNITS
    right = UNITS - left
    wide = out_weight.shape[1]
    far = halves(1 - half)
    its = lax.ppermute(far, "tp", cross)
    send, keep = out_product(far, out_weight, left, right)
    got = lax.ppermute(send, "tp", swap)
    crossed = lax.ppermute((got.astype(F32) + keep.astype(F32)).astype(BF16), "tp", cross)
    near = halves(half)
    send, keep = out_product(near, out_weight, 0, left, its, [piece_a, piece_b])
    got = lax.ppermute(send, "tp", swap)
    late_send, late_keep = out_product(near, out_weight, left, right)
    late_got = lax.ppermute(late_send, "tp", swap)
    out = final_sum(wide, 0, got, keep)
    return final_sum(wide, left * wide // UNITS, late_got, late_keep, crossed, into=out)


def solution(mesh):
    placed = (
        P("kv", None),
        P(None, "tp"),
        P(None, "tp"),
        P(None, "tp"),
        P(),
        P(),
        P(),
        P(),
        P("tp", None),
        P("kv", "tp", None),
    )
    count = mesh.shape["kv"]

    def body(*args):
        return local(count, mesh.shape["tp"], *args)

    return jax.shard_map(
        body, mesh=mesh, in_specs=placed, out_specs=P(("kv", "tp"), None), check_vma=False
    )
```

```python
import functools

import jax
import jax.numpy as jnp
from jax import lax
from jax.experimental import pallas as pl
from jax.experimental.pallas import tpu as pltpu
from jax.sharding import PartitionSpec as P


HD = 64
CMP = 32
SB = 64
N_SEL = 16
LANES = 2 * HD
SPAN_PAD = 32
UNITS = 16
BLOCK = 512
FIRST_LIMIT = 59 * 1024 * 1024
KV_AHEAD, Q_AHEAD = 4, 2
FIRST_UNITS, MORE_UNITS = 2, 7
LOW = -1e30
FLOOR = -1e29
EXP_SCALE = HD ** (-0.5) * 1.4426950408889634
VMEM_LIMIT = 60 * 1024 * 1024
SELECT_LIMIT = 8 * 1024 * 1024
ATTEND_LIMIT = 24 * 1024 * 1024
PROJ_LIMIT = 57 * 1024 * 1024
PROD_LIMIT = 16 * 1024 * 1024


F32 = jnp.float32
BF16 = jnp.bfloat16


def lane_iota(rows):
    return lax.broadcasted_iota(jnp.int32, (rows, LANES), 1)


def row_iota(rows):
    return lax.broadcasted_iota(jnp.int32, (rows, LANES), 0)


def staged(copies, ahead, step):
    for group in copies[:ahead]:
        for copy in group:
            copy.start()
    for i, group in enumerate(copies):
        for copy in group:
            copy.wait()
        if i + ahead < len(copies):
            for copy in copies[i + ahead]:
                copy.start()
        step(i)


def kv_kernel(part_ref, tok_ref, wk_ref, wv_ref, pos_hbm, km_hbm, vm_hbm, wo_ref, kv_out, sm_out, more_ref, tok, weight,
              acc_ref, held, pos_ref, km_ref, vm_ref, kv_ref, sm_ref, sems, wide_sems, small_sems):
    key_heads, rows = kv_ref.shape[0], kv_ref.shape[1]
    steps, chunk = weight.shape[0], weight.shape[1]
    at_v = key_heads * HD
    copies = []
    for i in range(steps):
        depth = slice(i * chunk, (i + 1) * chunk)
        copies.append(
            [
                pltpu.make_async_copy(tok_ref.at[:, depth], tok.at[i], sems.at[i, 0]),
                pltpu.make_async_copy(wk_ref.at[depth, :], weight.at[i, :, :at_v], sems.at[i, 1]),
                pltpu.make_async_copy(wv_ref.at[depth, :], weight.at[i, :, at_v:], sems.at[i, 2]),
            ]
        )

    unit = wo_ref.shape[1] // UNITS
    more = slice(2 * FIRST_UNITS * unit, (2 * FIRST_UNITS + MORE_UNITS) * unit)
    fetch = pltpu.make_async_copy(wo_ref.at[:, more], held, wide_sems.at[0])
    put = pltpu.make_async_copy(held, more_ref, wide_sems.at[1])

    small = [
        pltpu.make_async_copy(pos_hbm, pos_ref, small_sems.at[0]),
        pltpu.make_async_copy(km_hbm, km_ref, small_sems.at[1]),
        pltpu.make_async_copy(vm_hbm, vm_ref, small_sems.at[2]),
    ]

    def step(i):
        if i == 0:
            for copy in small:
                copy.start()
            fetch.start()
        piece = jnp.dot(tok[i], weight[i], preferred_element_type=F32)
        acc_ref[...] = piece if i == 0 else acc_ref[...] + piece

    staged(copies, KV_AHEAD, step)
    fetch.wait()
    put.start()
    for copy in small:
        copy.wait()
    low_half = lane_iota(rows) < HD
    spans = rows // CMP
    pos = pos_ref[...].astype(F32)
    pos = jnp.concatenate([pos, pos], axis=1)
    line = lax.broadcasted_iota(jnp.int32, km_ref.shape, 0)
    eye = lax.broadcasted_iota(jnp.int32, (CMP, CMP), 0) == lax.broadcasted_iota(jnp.int32, (CMP, CMP), 1)

    def column(ref, head):
        kept = jnp.sum(jnp.where(line == head, ref[...].astype(F32), 0.0), axis=0, keepdims=True)
        return jnp.sum(jnp.where(eye, kept, 0.0), axis=1, keepdims=True)

    outs = []
    for g in range(key_heads):
        k = acc_ref[:, (g // 2) * LANES : (g // 2 + 1) * LANES]
        v = acc_ref[:, at_v + (g // 2) * LANES : at_v + (g // 2 + 1) * LANES]
        if g % 2 == 0:
            both = jnp.where(low_half, k, pltpu.roll(v, HD, 1))
        else:
            both = jnp.where(low_half, pltpu.roll(k, HD, 1), v)
        both = both.astype(BF16)
        kv_ref[g] = both
        outs.append(pltpu.make_async_copy(kv_ref.at[g], kv_out.at[g], small_sems.at[3 + 2 * g]))
        outs[-1].start()
        head = part_ref[0] * key_heads + g
        mix = jnp.where(lane_iota(CMP) < HD, column(km_ref, head), column(vm_ref, head))
        windows = both.astype(F32).reshape(spans, CMP, LANES) + pos[None]
        total = jnp.sum(windows * mix[None], axis=1)
        pad = jnp.zeros((SPAN_PAD - spans, LANES), F32)
        sm_ref[g] = jnp.concatenate([total, pad], axis=0).astype(BF16)
        outs.append(pltpu.make_async_copy(sm_ref.at[g], sm_out.at[g], small_sems.at[4 + 2 * g]))
        outs[-1].start()
    for copy in outs:
        copy.wait()
    put.wait()


def project_kv(part, tokens, key_weight, value_weight, pos, kmix, vmix, out_weight):
    rows, depth = tokens.shape
    inner, wide = out_weight.shape
    width = key_weight.shape[1]
    key_heads = width // HD
    steps = 4
    chunk = depth // steps
    hbm = pl.BlockSpec(memory_space=pl.ANY)
    smem = pl.BlockSpec(memory_space=pltpu.SMEM)
    return pl.pallas_call(
        kv_kernel,
        in_specs=[smem] + [hbm] * 7,
        out_specs=[hbm] * 3,
        scratch_shapes=[
            pltpu.VMEM((steps, rows, chunk), BF16),
            pltpu.VMEM((steps, chunk, 2 * width), BF16),
            pltpu.VMEM((rows, 2 * width), F32),
            pltpu.VMEM((inner, MORE_UNITS * wide // UNITS), BF16),
            pltpu.VMEM(pos.shape, BF16),
            pltpu.VMEM(kmix.shape, BF16),
            pltpu.VMEM(vmix.shape, BF16),
            pltpu.VMEM((key_heads, rows, LANES), BF16),
            pltpu.VMEM((key_heads, SPAN_PAD, LANES), BF16),
            pltpu.SemaphoreType.DMA((steps, 3)),
            pltpu.SemaphoreType.DMA((2,)),
            pltpu.SemaphoreType.DMA((3 + 2 * key_heads,)),
        ],
        out_shape=[
            jax.ShapeDtypeStruct((key_heads, rows, LANES), BF16),
            jax.ShapeDtypeStruct((key_heads, SPAN_PAD, LANES), BF16),
            jax.ShapeDtypeStruct((inner, MORE_UNITS * wide // UNITS), BF16),
        ],
        cost_estimate=pl.CostEstimate(
            flops=4 * rows * depth * width, transcendentals=0, bytes_accessed=2 * depth * (rows + 2 * width)
        ),
        compiler_params=pltpu.CompilerParams(vmem_limit_bytes=VMEM_LIMIT),
        name="project_kv",
    )(part, tokens, key_weight, value_weight, pos, kmix, vmix, out_weight)


def q_kernel(part_ref, tok_ref, wq_ref, gw_ref, q_out, gate_out, tok, weight, gate_rows, acc_ref, gacc_ref, q_ref,
             gate_ref, sems, out_sems):
    heads, rows = q_ref.shape[0], q_ref.shape[1]
    gates = gate_ref.shape[1]
    steps, chunk = weight.shape[0], weight.shape[1]
    start = pl.multiple_of(part_ref[0] * gates, gates)
    copies = []
    for i in range(steps):
        depth = slice(i * chunk, (i + 1) * chunk)
        copies.append(
            [
                pltpu.make_async_copy(tok_ref.at[:, depth], tok.at[i], sems.at[i, 0]),
                pltpu.make_async_copy(wq_ref.at[depth, :], weight.at[i], sems.at[i, 1]),
                pltpu.make_async_copy(gw_ref.at[pl.ds(start, gates), depth], gate_rows.at[i], sems.at[i, 2]),
            ]
        )

    def step(i):
        piece = jnp.dot(tok[i], weight[i], preferred_element_type=F32)
        gpiece = lax.dot_general(tok[i], gate_rows[i], (((1,), (1,)), ((), ())), preferred_element_type=F32)
        acc_ref[...] = piece if i == 0 else acc_ref[...] + piece
        gacc_ref[...] = gpiece if i == 0 else gacc_ref[...] + gpiece

    staged(copies, Q_AHEAD, step)
    gate_ref[...] = jax.nn.sigmoid(gacc_ref[...])
    outs = [pltpu.make_async_copy(gate_ref, gate_out, out_sems.at[heads])]
    outs[0].start()
    lane, inner = lane_iota(rows), lax.rem(row_iota(rows), SB)
    low_half = lane < HD
    ext = jnp.where((lane == HD) | (lane - HD > inner), 1.0, 0.0)
    for h in range(heads):
        slab = acc_ref[:, (h // 2) * LANES : (h // 2 + 1) * LANES]
        if h % 2:
            slab = pltpu.roll(slab, HD, 1)
        q_ref[h] = jnp.where(low_half, slab, ext).astype(BF16)
        outs.append(pltpu.make_async_copy(q_ref.at[h], q_out.at[h], out_sems.at[h]))
        outs[-1].start()
    for copy in outs:
        copy.wait()


def project_q(part, tokens, query_weight, gate_rows):
    rows, depth = tokens.shape
    qwidth = query_weight.shape[1]
    heads = qwidth // HD
    steps = 4
    chunk = depth // steps
    hbm = pl.BlockSpec(memory_space=pl.ANY)
    smem = pl.BlockSpec(memory_space=pltpu.SMEM)
    return pl.pallas_call(
        q_kernel,
        in_specs=[smem, hbm, hbm, hbm],
        out_specs=[hbm, hbm],
        scratch_shapes=[
            pltpu.VMEM((steps, rows, chunk), BF16),
            pltpu.VMEM((steps, chunk, qwidth), BF16),
            pltpu.VMEM((steps, 2 * heads, chunk), BF16),
            pltpu.VMEM((rows, qwidth), F32),
            pltpu.VMEM((rows, 2 * heads), F32),
            pltpu.VMEM((heads, rows, LANES), BF16),
            pltpu.VMEM((rows, 2 * heads), F32),
            pltpu.SemaphoreType.DMA((steps, 3)),
            pltpu.SemaphoreType.DMA((heads + 1,)),
        ],
        out_shape=[
            jax.ShapeDtypeStruct((heads, rows, LANES), BF16),
            jax.ShapeDtypeStruct((rows, 2 * heads), F32),
        ],
        cost_estimate=pl.CostEstimate(
            flops=3 * rows * depth * qwidth, transcendentals=0, bytes_accessed=2 * depth * (rows + qwidth)
        ),
        compiler_params=pltpu.CompilerParams(vmem_limit_bytes=PROJ_LIMIT),
        name="project_q",
    )(part, tokens, query_weight, gate_rows)


def copy_kernel(odd_ref, from_ref, to_ref, sem):
    width = to_ref.shape[1]
    columns = pl.ds(pl.multiple_of(odd_ref[0] * width, width), width)
    copy = pltpu.make_async_copy(from_ref.at[:, columns], to_ref, sem)
    copy.start()
    copy.wait()


def first_piece(odd, out_weight):
    inner, wide = out_weight.shape
    width = FIRST_UNITS * wide // UNITS
    return pl.pallas_call(
        copy_kernel,
        in_specs=[pl.BlockSpec(memory_space=pltpu.SMEM), pl.BlockSpec(memory_space=pl.ANY)],
        out_specs=pl.BlockSpec(memory_space=pltpu.VMEM),
        out_shape=jax.ShapeDtypeStruct((inner, width), BF16),
        scratch_shapes=[pltpu.SemaphoreType.DMA],
        compiler_params=pltpu.CompilerParams(vmem_limit_bytes=FIRST_LIMIT),
        name="first_piece",
    )(odd, out_weight)


def select_kernel(count, own_ref, req_ref, kv_ref, sm_ref, *out_refs):
    heads = kv_ref.shape[0]
    own = own_ref[0]
    for shift in range(1, count):
        taker = jnp.minimum(own + shift, count - 1)
        out_ref = out_refs[shift - 1]
        for g in range(heads):
            for j in range(2):
                block = req_ref[taker, own * (2 * heads) + 2 * g + j]
                out_ref[g, j * SB : (j + 1) * SB, :] = kv_ref[g, pl.ds(pl.multiple_of(block * SB, SB), SB), :]
            out_ref[g, 2 * SB :, :] = sm_ref[g]


def select_blocks(count, own, requests, kv, summaries):
    heads = kv.shape[0]
    piece = (heads, 2 * SB + SPAN_PAD, LANES)
    smem = pl.BlockSpec(memory_space=pltpu.SMEM)
    full = lambda shape: pl.BlockSpec(shape, lambda i: (0,) * len(shape))
    return pl.pallas_call(
        functools.partial(select_kernel, count),
        grid=(1,),
        in_specs=[smem, smem, full(kv.shape), full(summaries.shape)],
        out_specs=[full(piece)] * (count - 1),
        out_shape=[jax.ShapeDtypeStruct(piece, BF16)] * (count - 1),
        compiler_params=pltpu.CompilerParams(vmem_limit_bytes=SELECT_LIMIT),
        name="select_blocks",
    )(own, requests, kv, summaries)


def stage_kernel(q_ref, gate_ref, q_out, gate_out, sems):
    copies = [pltpu.make_async_copy(q_ref, q_out, sems.at[0]), pltpu.make_async_copy(gate_ref, gate_out, sems.at[1])]
    for copy in copies:
        copy.start()
    for copy in copies:
        copy.wait()


def bring(q, gates):
    hbm = pl.BlockSpec(memory_space=pl.ANY)
    vmem = pl.BlockSpec(memory_space=pltpu.VMEM)
    return pl.pallas_call(
        stage_kernel,
        in_specs=[hbm, hbm],
        out_specs=[vmem, vmem],
        out_shape=[jax.ShapeDtypeStruct(q.shape, BF16), jax.ShapeDtypeStruct(gates.shape, F32)],
        scratch_shapes=[pltpu.SemaphoreType.DMA((2,))],
        compiler_params=pltpu.CompilerParams(vmem_limit_bytes=SELECT_LIMIT),
        name="stage",
    )(q, gates)


def attn_kernel(count, blocks, *refs):
    half_ref, own_ref, core_ref, table_ref, q_ref, gate_ref, kv_ref, sm_ref = refs[:8]
    recv_refs = refs[8 : 8 + count - 1]
    out_ref, poolk, poolv, sumk, sumv, score0, score1, weight0, weight1 = refs[8 + count - 1 :]
    own, base = own_ref[0], half_ref[0] * blocks
    turn = (1 - core_ref[0]) * (blocks * SB // 2)
    heads, rows = kv_ref.shape[0], kv_ref.shape[1]
    group = q_ref.shape[0] // heads
    own_blocks = rows // SB
    spans = rows // CMP
    total_blocks = poolk.shape[1] - 1
    named = N_SEL * SB
    lane, row = lane_iota(SB), row_iota(SB)
    keep = jnp.where(lane < HD, 1.0, 0.0).astype(BF16)
    other = jnp.where(lane < HD, 0.0, 1.0).astype(BF16)
    span_lane, span_row = lane_iota(SPAN_PAD), row_iota(SPAN_PAD)
    low_half = lane < HD
    diagonal = jnp.where((lane - HD == row) & (row > 0), LOW, 0.0).astype(BF16)
    contract = (((1,), (1,)), ((), ()))

    def wide(piece):
        n = piece.shape[0]
        turned = pltpu.roll(piece.astype(F32), HD, 1).astype(BF16)
        return jnp.concatenate([piece * other[:n] + keep[:n], turned * keep[:n] + other[:n]], axis=1)

    for g in range(heads):
        for j in range(own_blocks):
            piece = kv_ref[g, j * SB : (j + 1) * SB, :]
            poolk[g, j] = piece * keep
            poolv[g, j] = wide(piece)
        for k, recv in enumerate(recv_refs):
            for j in range(2):
                piece = recv[g, j * SB : (j + 1) * SB, :]
                poolk[g, own_blocks + 2 * k + j] = piece * keep
                poolv[g, own_blocks + 2 * k + j] = wide(piece)
        poolk[g, total_blocks] = jnp.where(lane == HD, LOW, 0.0).astype(BF16)
        poolv[g, total_blocks] = jnp.zeros((SB, 2 * LANES), BF16)
        for k in range(count):
            piece = sm_ref[g] if k == 0 else recv_refs[k - 1][g, 2 * SB :, :]
            sumv[g, k * SPAN_PAD : (k + 1) * SPAN_PAD] = wide(piece)
            if k:
                hidden = (span_lane == HD) & ((span_row >= spans) | (own < k))
                bias = jnp.where(hidden, LOW, 0.0).astype(BF16)
                sumk[g, (k - 1) * SPAN_PAD : k * SPAN_PAD] = piece * keep[:SPAN_PAD] + bias

    def scores(j, g, score):
        block = base + j
        last = SB // CMP * block
        hidden = (span_lane == HD) & (span_row >= last + SB // CMP)
        for i in range(SB // CMP):
            hidden = hidden | ((span_row == last + i) & (span_lane == HD + (i + 1) * CMP - 1))
        bias = jnp.where(hidden, LOW, 0.0).astype(BF16)
        pieces = [poolk[g, table_ref[block, g * N_SEL + s]] for s in range(N_SEL)]
        pieces[0] = pieces[0] + diagonal
        keys = jnp.concatenate([*pieces, sm_ref[g] * keep[:SPAN_PAD] + bias, sumk[g]], axis=0)
        q = q_ref[g * group : (g + 1) * group, pl.ds(pl.multiple_of(j * SB, SB), SB), :]
        q = q.reshape(group * SB, LANES)
        score[...] = lax.dot_general(q, keys, contract, preferred_element_type=F32)

    def weights(score, weight):
        top = jnp.max(score[:, :named], axis=1, keepdims=True)
        weight[:, :named] = jnp.exp2((score[:, :named] - top) * EXP_SCALE).astype(BF16)
        top = jnp.maximum(jnp.max(score[:, named:], axis=1, keepdims=True), FLOOR)
        weight[:, named:] = jnp.exp2((score[:, named:] - top) * EXP_SCALE).astype(BF16)

    def mixed(j, g, weight):
        block = base + j
        values = jnp.concatenate([poolv[g, table_ref[block, g * N_SEL + s]] for s in range(N_SEL)], axis=0)
        picked = jnp.dot(weight[:, :named], values, preferred_element_type=F32)
        summed = jnp.dot(weight[:, named:], sumv[g], preferred_element_type=F32)
        gate = gate_ref[pl.ds(pl.multiple_of(j * SB, SB), SB), :]
        for pair in range(group // 2):
            h = g * group + 2 * pair
            even, odd = slice(2 * pair * SB, (2 * pair + 1) * SB), slice((2 * pair + 1) * SB, (2 * pair + 2) * SB)

            def branch(out, which):
                top = jnp.where(low_half, out[even, LANES:], out[odd, :LANES])
                total = jnp.where(low_half, out[even, :LANES], out[odd, LANES:])
                scale = jnp.where(low_half, gate[:, 2 * h + which : 2 * h + which + 1],
                                  gate[:, 2 * h + 2 + which : 2 * h + 3 + which])
                return top * (scale / jnp.maximum(total, 1e-30))

            both = (branch(summed, 0) + branch(picked, 1)).astype(BF16)
            at = (g * group) // 2 + pair
            for part in range(SB // CMP):
                place = lax.rem(j * SB + part * CMP + turn, blocks * SB)
                place = pl.ds(pl.multiple_of(place, CMP), CMP)
                out_ref[place, at * LANES : (at + 1) * LANES] = both[part * CMP : (part + 1) * CMP]

    slots = [(score0, weight0), (score1, weight1)]

    def stage(first, ahead, behind):
        if first is not None:
            scores(*first, slots[first[1] % 2][0])
        if ahead is not None:
            weights(*slots[ahead[1] % 2])
        if behind is not None:
            mixed(*behind, slots[behind[1] % 2][1])

    def unit(j, g):
        return (j + g // heads, g % heads) if g >= 0 else (j - 1, g + heads)

    stage(unit(0, 0), None, None)
    stage(unit(0, 1), unit(0, 0), None)

    def body(j, carry):
        for g in range(heads):
            stage(unit(j, g), unit(j, g - 1), unit(j, g - 2))
        return carry

    lax.fori_loop(1, blocks, body, 0)
    stage(None, unit(blocks - 1, 1), unit(blocks - 1, 0))
    stage(None, None, unit(blocks - 1, 1))


def attend(count, blocks, half, own, core, table, q, gates, kv, summaries, received):
    heads, rows = kv.shape[0], kv.shape[1]
    group = q.shape[0] // heads
    total = rows // SB + 2 * (count - 1)
    keys = N_SEL * SB + count * SPAN_PAD
    full = lambda shape: pl.BlockSpec(shape, lambda i, *s: (0,) * len(shape))
    return pl.pallas_call(
        functools.partial(attn_kernel, count, blocks),
        grid_spec=pltpu.PrefetchScalarGridSpec(
            num_scalar_prefetch=4,
            grid=(1,),
            in_specs=[
                pl.BlockSpec((q.shape[0], blocks * SB, LANES), lambda i, half, *s: (0, half[0], 0)),
                pl.BlockSpec((blocks * SB, gates.shape[1]), lambda i, half, *s: (half[0], 0)),
                full(kv.shape),
                full(summaries.shape),
                *[full(r.shape) for r in received],
            ],
            out_specs=full((blocks * SB, q.shape[0] * HD)),
        scratch_shapes=[
            pltpu.VMEM((heads, total + 1, SB, LANES), BF16),
            pltpu.VMEM((heads, total + 1, SB, 2 * LANES), BF16),
            pltpu.VMEM((heads, (count - 1) * SPAN_PAD, LANES), BF16),
            pltpu.VMEM((heads, count * SPAN_PAD, 2 * LANES), BF16),
            pltpu.VMEM((group * SB, keys), F32),
            pltpu.VMEM((group * SB, keys), F32),
            pltpu.VMEM((group * SB, keys), BF16),
            pltpu.VMEM((group * SB, keys), BF16),
        ]),
        out_shape=jax.ShapeDtypeStruct((blocks * SB, q.shape[0] * HD), BF16),
        cost_estimate=pl.CostEstimate(
            flops=blocks * q.shape[0] * SB * keys * LANES * 4,
            transcendentals=blocks * q.shape[0] * SB * keys,
            bytes_accessed=4 * kv.size,
        ),
        compiler_params=pltpu.CompilerParams(vmem_limit_bytes=ATTEND_LIMIT),
        name="attend",
    )(half, own, core, table, q, gates, kv, summaries, *received)


def product_kernel(first, near_ref, own_ref, send_ref, keep_ref):
    rows, width = send_ref.shape
    for at in range(0, width, BLOCK):
        size = min(BLOCK, width - at)
        total = jnp.dot(near_ref[...], own_ref[:, first + at : first + at + size], preferred_element_type=F32)
        send_ref[:, at : at + size] = total[:rows].astype(BF16)
        keep_ref[:, at : at + size] = total[rows:].astype(BF16)


def joint_kernel(odd_ref, near_ref, its_ref, own_ref, a_ref, b_ref, d_ref, send_ref, keep_ref, other, sems):
    rows, width = send_ref.shape
    width_a = a_ref.shape[1]
    near_at = pl.multiple_of(odd_ref[0] * width_a, width_a)
    far_at = pl.multiple_of((1 - odd_ref[0]) * width_a, width_a)
    copies = [
        pltpu.make_async_copy(a_ref, other.at[:, pl.ds(near_at, width_a)], sems.at[0]),
        pltpu.make_async_copy(d_ref, other.at[:, pl.ds(far_at, width_a)], sems.at[1]),
        pltpu.make_async_copy(b_ref, other.at[:, 2 * width_a :], sems.at[2]),
    ]
    for copy in copies:
        copy.start()
    for at in range(0, width, BLOCK):
        size = min(BLOCK, width - at)
        columns = slice(at, at + size)
        total = jnp.dot(near_ref[...], own_ref[:, columns], preferred_element_type=F32)
        if at == 0:
            copies[0].wait()
            copies[1].wait()
        if at == 2 * width_a // BLOCK * BLOCK:
            copies[2].wait()
        total += jnp.dot(its_ref[...], other[:, columns], preferred_element_type=F32)
        send_ref[:, columns] = total[:rows].astype(BF16)
        keep_ref[:, columns] = total[rows:].astype(BF16)


def out_product(near, out_weight, first, units, odd=None, its=None, pieces=()):
    depth, wide = out_weight.shape
    unit = wide // UNITS
    rows = near.shape[0] // 2
    width = units * unit
    full = lambda shape: pl.BlockSpec(shape, lambda i: (0,) * len(shape))
    hbm = pl.BlockSpec(memory_space=pl.ANY)
    vmem = pl.BlockSpec(memory_space=pltpu.VMEM)
    common = dict(
        grid=(1,),
        out_specs=[full((rows, width))] * 2,
        out_shape=[jax.ShapeDtypeStruct((rows, width), BF16)] * 2,
        cost_estimate=pl.CostEstimate(flops=8 * rows * depth * width, transcendentals=0, bytes_accessed=4 * depth * width),
        compiler_params=pltpu.CompilerParams(vmem_limit_bytes=PROD_LIMIT),
    )
    if not pieces:
        return pl.pallas_call(
            functools.partial(product_kernel, first * unit),
            in_specs=[full(near.shape), vmem],
            name="out_product",
            **common,
        )(near, out_weight)
    return pl.pallas_call(
        joint_kernel,
        in_specs=[pl.BlockSpec(memory_space=pltpu.SMEM), full(near.shape), full(its.shape), vmem, hbm, hbm, hbm],
        scratch_shapes=[pltpu.VMEM((depth, width), BF16), pltpu.SemaphoreType.DMA((3,))],
        name="joint_product",
        **common,
    )(odd, near, its, out_weight, *pieces)


def final_kernel(first, *refs):
    out_ref, total, sem = refs[-3:]
    width = total.shape[1]
    value = refs[0][...].astype(F32) + refs[1][...].astype(F32)
    if len(refs) > 6:
        value += refs[2][...].astype(F32)
    total[...] = value.astype(BF16)
    copy = pltpu.make_async_copy(total, out_ref.at[:, first : first + width], sem)
    copy.start()
    copy.wait()


def final_sum(wide, first, *parts, into=None):
    rows, width = parts[0].shape
    full = pl.BlockSpec((rows, width), lambda i: (0, 0))
    hbm = pl.BlockSpec(memory_space=pl.ANY)
    more = [] if into is None else [into]
    return pl.pallas_call(
        functools.partial(final_kernel, first),
        grid=(1,),
        in_specs=[full] * len(parts) + [hbm] * len(more),
        out_specs=hbm,
        out_shape=jax.ShapeDtypeStruct((rows, wide), BF16),
        scratch_shapes=[pltpu.VMEM((rows, width), BF16), pltpu.SemaphoreType.DMA],
        input_output_aliases={} if into is None else {len(parts): 0},
        compiler_params=pltpu.CompilerParams(vmem_limit_bytes=PROD_LIMIT),
        name="final_sum",
    )(*parts, *more)


def local(count, parts, tokens, query_weight, key_weight, value_weight, gate_weight, summary_pos, key_mixing,
          value_mixing, out_weight, chosen):
    rows = tokens.shape[0]
    own = lax.axis_index("kv").astype(jnp.int32)
    part = lax.axis_index("tp").astype(jnp.int32)
    own_blocks = rows // SB
    heads = key_weight.shape[1] // HD
    own1, part1, odd1 = own.reshape(1), part.reshape(1), (own % 2).reshape(1)

    source = chosen // own_blocks
    place = chosen - source * own_blocks
    match = source[None] == jnp.arange(count, dtype=jnp.int32)[:, None, None, None]
    lowest = jnp.min(jnp.where(match, place[None], own_blocks - 1), axis=(1, 3))
    highest = jnp.max(jnp.where(match, place[None], 0), axis=(1, 3))
    request = jnp.stack([lowest, highest], axis=-1).reshape(1, count * heads * 2)
    everyone = jnp.where(jnp.arange(count, dtype=jnp.int32)[:, None] == own, request, 0)
    if count & (count - 1) == 0:
        bit = 1
        while bit < count:
            got = lax.ppermute(everyone, "kv", [(i, i ^ bit) for i in range(count)])
            everyone = everyone + got
            if 4 * bit == count:
                chosen = lax.optimization_barrier((chosen, got))[0]
            bit = 2 * bit
    else:
        everyone = lax.all_gather(request, "kv", axis=0, tiled=True)

    cross = [(i, i ^ 2) for i in range(parts)]
    swap = [(i, i ^ 1) for i in range(parts)]
    piece_a = lax.ppermute(first_piece(odd1, out_weight), "tp", cross)
    kv, summaries, more = project_kv(
        part1, tokens, key_weight, value_weight, summary_pos, key_mixing.T, value_mixing.T, out_weight
    )
    q, gates = project_q(part1, tokens, query_weight, gate_weight.T)
    piece_b = lax.ppermute(more, "tp", cross)

    pieces = select_blocks(count, own1, everyone, kv, summaries)
    received = []
    for k in range(1, count):
        received.append(lax.ppermute(pieces[k - 1], "kv", [(i, i + k) for i in range(count - k)]))

    source = chosen // own_blocks
    place = chosen - source * own_blocks
    match = source[None] == jnp.arange(count, dtype=jnp.int32)[:, None, None, None]

    q, gates = bring(q, gates)

    high_at = jnp.sum(jnp.where(match, highest[:, None, :, None], 0), axis=0)
    away = own_blocks + 2 * (own - source - 1) + (place == high_at).astype(jnp.int32)
    index = jnp.where(source == own, place, away)
    slots = jnp.arange(N_SEL, dtype=jnp.int32)
    earlier = slots[None, :] < slots[:, None]
    repeated = jnp.any((chosen[..., :, None] == chosen[..., None, :]) & earlier, axis=-1)
    first = jnp.logical_not(repeated)
    rank = jnp.sum((first[..., None, :] & earlier).astype(jnp.int32), axis=-1)
    at = (rank[..., None, :] == slots[:, None]) & first[..., None, :]
    fill = own_blocks + 2 * (count - 1)
    table = jnp.where(jnp.any(at, axis=-1), jnp.sum(jnp.where(at, index[..., None, :], 0), axis=-1), fill)
    table = table.reshape(own_blocks, heads * N_SEL)

    half_blocks = own_blocks // 2
    half = part // 2
    core1 = (part % 2).reshape(1)

    def halves(which):
        return attend(count, half_blocks, which.reshape(1), own1, core1, table, q, gates, kv, summaries,
                      received)

    left = 2 * FIRST_UNITS + MORE_UNITS
    right = UNITS - left
    wide = out_weight.shape[1]
    piece_d = lax.ppermute(piece_a, "kv", [(i, i ^ 1) for i in range(count)])
    far = halves(1 - half)
    its = lax.ppermute(far, "tp", cross)
    send, keep = out_product(far, out_weight, left, right)
    got = lax.ppermute(send, "tp", swap)
    crossed = lax.ppermute((got.astype(F32) + keep.astype(F32)).astype(BF16), "tp", cross)
    near = halves(half)
    send, keep = out_product(near, out_weight, 0, left, odd1, its, [piece_a, piece_b, piece_d])
    got = lax.ppermute(send, "tp", swap)
    late_send, late_keep = out_product(near, out_weight, left, right)
    late_got = lax.ppermute(late_send, "tp", swap)
    out = final_sum(wide, 0, got, keep)
    return final_sum(wide, left * wide // UNITS, late_got, late_keep, crossed, into=out)


def solution(mesh):
    placed = (
        P("kv", None),
        P(None, "tp"),
        P(None, "tp"),
        P(None, "tp"),
        P(),
        P(),
        P(),
        P(),
        P("tp", None),
        P("kv", "tp", None),
    )
    count = mesh.shape["kv"]

    def body(*args):
        return local(count, mesh.shape["tp"], *args)

    return jax.shard_map(
        body, mesh=mesh, in_specs=placed, out_specs=P(("kv", "tp"), None), check_vma=False
    )
```
